32 devices in a mesh: ep: 8 (over z, x), tp: 4 (over y, core).
Axes of the slice: x: 2, y: 2, z: 4, core: 2. Of those that a mesh axis runs over, the one named last changes fastest.
Arguments:
- mixer_input: bfloat16 [4096, 2048], P(('ep', 'tp')), may hold values from -6 to 6
- log_decay: float32 [4096, 8], P('ep', 'tp'), may hold values from -0.8 to 0
- mixer_gain: float32 [2048], replicated, may hold values from 0.1 to 1.9
- query_weight: bfloat16 [2048, 1024], P(None, 'tp'), may hold values from -0.125 to 0.125
- key_weight: bfloat16 [2048, 1024], P(None, 'tp'), may hold values from -0.125 to 0.125
- value_weight: bfloat16 [2048, 2048], P(None, 'tp'), may hold values from -0.125 to 0.125
- gate_weight: bfloat16 [2048, 2048], P(None, 'tp'), may hold values from -0.125 to 0.125
- head_gain: float32 [2048], P('tp'), may hold values from 0.1 to 1.9
- output_weight: bfloat16 [2048, 2048], P('tp'), may hold values from -0.125 to 0.125
- expert_input: bfloat16 [4096, 2048], P(('ep', 'tp')), may hold values from -6 to 6
- expert_gain: float32 [2048], replicated, may hold values from 0.1 to 1.9
- routes: int32 [4096, 2], P(('ep', 'tp')), may hold values from 0 to 31, as said below
- group_weight: float32 [4096], P(('ep', 'tp')), may hold values from 0.3 to 1
- pair_weight: float32 [4096, 2], P(('ep', 'tp')), may hold values from 0.2 to 1
- expert_gate: bfloat16 [32, 2048, 1024], P(('ep', 'tp')), may hold values from -0.125 to 0.125
- expert_up: bfloat16 [32, 2048, 1024], P(('ep', 'tp')), may hold values from -0.125 to 0.125
- expert_down: bfloat16 [32, 1024, 2048], P(('ep', 'tp')), may hold values from -0.1875 to 0.1875
Outputs:
- mixer_output: bfloat16 [4096, 2048], P(('ep', 'tp'))
- expert_output: bfloat16 [4096, 2048], P(('ep', 'tp'))
The draws below stay inside these ranges and needn't reach their ends.
Inputs may be any that keep to these rules, and one draw needn't show every extreme that they name: `routes`: in the rows of one device each expert is named at most 12 times; one expert is named exactly 12 times in the rows of every device. A row names two different experts of the same group, a group being 8 consecutive expert numbers.
All inputs are finite; a program needn't handle non-finite values.
Results may differ from the reference program's by a relative error of at most 0.023.
Values may be sent and summed in bfloat16 or wider, within the bound.
A program may use at most 128 MiB of HBM per device.

```python
import jax
import jax.numpy as jnp
from jax import lax

D = 2048
RETENTION_HEADS = 8
KEY_DIM = 128
VALUE_DIM = 256
SPAN = 512
FF = 1024
GROUPS = 4
TOPK = 2
TOK_B = 128
KEY_WIDTH = 1024
VALUE_WIDTH = 2048
SEG_ROWS = 512
FIRST_POSITIONS = 4096
TOKENS_B = 4096
EXPERTS = 32
GROUP_SIZE = 8
CAP = 12
N_EP = 8
N_TP = 4


def draw_log_decay(key, part):
    split_random_keys = jax.random.split(jax.random.fold_in(key, 3), 7)
    fast_share = 0.5
    fast_heads = jax.random.uniform(split_random_keys[0], (RETENTION_HEADS,)) < fast_share
    fast_rate = 1.0 / jax.random.uniform(split_random_keys[1], (RETENTION_HEADS,), minval=30.0, maxval=100.0)
    slow_rate = jax.random.uniform(split_random_keys[2], (RETENTION_HEADS,), minval=0.1, maxval=0.5) / FIRST_POSITIONS
    head_rate = jnp.where(fast_heads, fast_rate, slow_rate)
    segments = FIRST_POSITIONS // SEG_ROWS
    segment_scale = jnp.exp(jax.random.uniform(split_random_keys[3], (segments,), minval=-0.7, maxval=0.7))
    row_scale = jnp.repeat(segment_scale, SEG_ROWS)
    jitter = jax.random.uniform(split_random_keys[4], (FIRST_POSITIONS, RETENTION_HEADS), minval=0.5, maxval=1.5)
    decay_factor = -head_rate[None, :] * row_scale[:, None] * jitter
    spike_rows = jax.random.randint(split_random_keys[5], (2,), 0, FIRST_POSITIONS)
    spike_loss = jnp.log(jax.random.uniform(split_random_keys[6], (2, RETENTION_HEADS), minval=0.5, maxval=0.8))
    position_list = jnp.arange(FIRST_POSITIONS)
    for index_value in range(2):
        decay_factor = decay_factor + jnp.where(position_list[:, None] == spike_rows[index_value], spike_loss[index_value][None, :], 0.0)
    return decay_factor.astype(jnp.float32)


def draw_routes(key, part):
    base_key = jax.random.fold_in(key, 7)
    chosen_key, block_base = jax.random.split(base_key)
    full_expert = jax.random.randint(chosen_key, (), 0, EXPERTS)
    pair_count = EXPERTS // 2

    def one_block(block_key):
        split_random_keys = jax.random.split(block_key, GROUPS + 3)
        orders = jnp.stack([jax.random.permutation(split_random_keys[group], GROUP_SIZE) for group in range(GROUPS)])
        labels = (orders + GROUP_SIZE * jnp.arange(GROUPS)[:, None]).reshape(-1).astype(jnp.int32)
        location = jnp.argmax(labels == full_expert)
        full_pair = location // 2
        slot_pairs = jnp.repeat(jnp.arange(pair_count), CAP)
        rank_order = jax.random.permutation(split_random_keys[GROUPS], pair_count * CAP)
        scores = jnp.where(slot_pairs == full_pair, rank_order, rank_order + pair_count * CAP)
        picked = jnp.argsort(scores)[:TOK_B]
        token_pairs = slot_pairs[picked][jax.random.permutation(split_random_keys[GROUPS + 1], TOK_B)]
        swapped = jax.random.randint(split_random_keys[GROUPS + 2], (TOK_B,), 0, 2)
        first_id = labels[2 * token_pairs + swapped]
        second = labels[2 * token_pairs + 1 - swapped]
        return jnp.stack([first_id, second], axis=1)
    block_keys = jax.random.split(block_base, TOKENS_B // TOK_B)
    return jax.vmap(one_block)(block_keys).reshape(TOKENS_B, TOPK).astype(jnp.int32)


def block_levels(key, extent, cuts, smallest, top_value):
    def one(dim, parts):
        draws = jax.random.uniform(jax.random.fold_in(jax.random.fold_in(key, 6), dim), (parts,), jnp.float32, smallest / len(cuts), top_value / len(cuts))
        return jnp.repeat(jnp.exp(draws), extent[dim] // parts).reshape((-1,) + (1,) * (len(extent) - dim - 1))

    loudness = one(*cuts[0])
    for cut in cuts[1:]:
        loudness = loudness * one(*cut)
    return loudness


def noise(key, shape, scale, reach, cuts=(), held_as=jnp.bfloat16):
    entries = jax.random.normal(key, shape, jnp.float32) * scale
    if len(cuts) > 0:
        entries = block_levels(key, shape, cuts, -0.22, 0.18) * entries
    return jnp.clip(entries, min=-reach, max=reach).astype(held_as)


def setup_inputs(seed: int = 0) -> dict:
    arg_keys = jax.random.split(jax.random.key(seed), 18)
    mixer_input = noise(arg_keys[0], (FIRST_POSITIONS, D), 1.0, 6.0, ((0, 32),))
    log_decay = draw_log_decay(jax.random.fold_in(arg_keys[17], 71), 0)
    mixer_gain = jnp.clip(1.0 + 0.18 * jax.random.normal(arg_keys[2], (D,), jnp.float32), 0.1, 1.9)
    query_weight = noise(arg_keys[3], (D, KEY_WIDTH), D ** -0.5, 0.125, ((1, 4),))
    key_weight = noise(arg_keys[4], (D, KEY_WIDTH), D ** -0.5, 0.125, ((1, 4),))
    value_weight = noise(arg_keys[5], (D, VALUE_WIDTH), D ** -0.5, 0.125, ((1, 4),))
    gate_weight = noise(arg_keys[6], (D, VALUE_WIDTH), D ** -0.5, 0.125, ((1, 4),))
    head_gain = jnp.clip(1.0 + 0.18 * jax.random.normal(arg_keys[7], (VALUE_WIDTH,), jnp.float32), 0.1, 1.9)
    output_weight = noise(arg_keys[8], (VALUE_WIDTH, D), VALUE_WIDTH ** -0.5, 0.125, ((0, 4),))
    expert_input = noise(arg_keys[9], (TOKENS_B, D), 1.0, 6.0, ((0, 32),))
    expert_gain = jnp.clip(1.0 + 0.18 * jax.random.normal(arg_keys[10], (D,), jnp.float32), 0.1, 1.9)
    routes = draw_routes(jax.random.fold_in(arg_keys[17], 71), 0)
    group_weight = jnp.clip(0.3 + 0.7 * jax.random.uniform(arg_keys[12], (TOKENS_B,), jnp.float32) ** block_levels(arg_keys[12], (TOKENS_B,), ((0, 32),), -0.2, 0.2), 0.3, 1.0)
    pair_weight = jnp.clip(0.2 + 0.8 * jax.random.uniform(arg_keys[13], (TOKENS_B, TOPK), jnp.float32) ** block_levels(arg_keys[13], (TOKENS_B, TOPK), ((0, 32),), -0.2, 0.2), 0.2, 1.0)
    expert_gate = noise(arg_keys[14], (EXPERTS, D, FF), D ** -0.5, 0.125, ((0, 32),))
    expert_up = noise(arg_keys[15], (EXPERTS, D, FF), D ** -0.5, 0.125, ((0, 32),))
    expert_down = noise(arg_keys[16], (EXPERTS, FF, D), FF ** -0.5, 0.1875, ((0, 32),))
    return dict(mixer_input=mixer_input, log_decay=log_decay, mixer_gain=mixer_gain, query_weight=query_weight, key_weight=key_weight, value_weight=value_weight, gate_weight=gate_weight, head_gain=head_gain, output_weight=output_weight, expert_input=expert_input, expert_gain=expert_gain, routes=routes, group_weight=group_weight, pair_weight=pair_weight, expert_gate=expert_gate, expert_up=expert_up, expert_down=expert_down)


EPSILON = 1e-05
THETA = 10000.0

def layer_norm(matrix, norm_gain):
    matrix = matrix.astype(jnp.float32)
    average = lax.optimization_barrier(jnp.mean(matrix, axis=-1, keepdims=True))
    centred = matrix - average
    spread = lax.optimization_barrier(jnp.mean(centred * centred, axis=-1, keepdims=True))
    return centred * lax.rsqrt(spread + EPSILON) * norm_gain.astype(jnp.float32)

def rotate(values, position):
    halfway = values.shape[-1] // 2
    frequency = THETA ** (-jnp.arange(halfway, dtype=jnp.float32) / halfway)
    angles = position[:, None] * frequency[None, :]
    cosine = jnp.cos(angles)[:, None, :]
    sine_part = jnp.sin(angles)[:, None, :]
    leading = values[..., :halfway]
    trailing = values[..., halfway:]
    return jnp.concatenate([leading * cosine - trailing * sine_part, trailing * cosine + leading * sine_part], axis=-1)

def block_step(state, inputs):
    query_rows, key_rows, value_rows, decay_factor = inputs
    span_len = query_rows.shape[0]
    cumulative = jnp.cumsum(decay_factor, axis=0)
    causal = jnp.arange(span_len)[:, None] >= jnp.arange(span_len)[None, :]
    log_gaps = cumulative.T[:, :, None] - cumulative.T[:, None, :]
    weight = jnp.where(causal[None], jnp.exp(jnp.minimum(log_gaps, 0.0)), 0.0)
    query_float = query_rows.astype(jnp.float32)
    key_float = key_rows.astype(jnp.float32)
    value_float = value_rows.astype(jnp.float32)
    scores = jnp.einsum('thd,shd->hts', query_float, key_float, precision=lax.Precision.HIGHEST)
    decayed = (scores * weight).astype(jnp.bfloat16).astype(jnp.float32)
    within = jnp.einsum('hts,she->the', decayed, value_float, precision=lax.Precision.HIGHEST)
    scaled = query_float * jnp.exp(cumulative)[:, :, None]
    carried = jnp.einsum('thd,hde->the', scaled, state, precision=lax.Precision.HIGHEST)
    span_total = cumulative[-1]
    remain = jnp.exp(span_total[None, :] - cumulative)
    update = jnp.einsum('shd,she->hde', key_float * remain[:, :, None], value_float, precision=lax.Precision.HIGHEST)
    return (state * jnp.exp(span_total)[:, None, None] + update, within + carried)

def token_mixer(mixer_input, log_decay, mixer_gain, query_weight, key_weight, value_weight, gate_weight, head_gain, output_weight):
    normed = layer_norm(mixer_input, mixer_gain).astype(jnp.bfloat16)

    def project(weight):
        return jnp.dot(normed, weight, preferred_element_type=jnp.float32).astype(jnp.bfloat16)
    query = project(query_weight).reshape(FIRST_POSITIONS, RETENTION_HEADS, KEY_DIM)
    keys_all = project(key_weight).reshape(FIRST_POSITIONS, RETENTION_HEADS, KEY_DIM)
    value = project(value_weight).reshape(FIRST_POSITIONS, RETENTION_HEADS, VALUE_DIM)
    gate = project(gate_weight).astype(jnp.float32)
    position = jnp.arange(FIRST_POSITIONS).astype(jnp.float32)
    rot_query = rotate(query.astype(jnp.float32), position).astype(jnp.bfloat16)
    rot_key = rotate(keys_all.astype(jnp.float32), position).astype(jnp.bfloat16)
    blocks = FIRST_POSITIONS // SPAN

    def split_blocks(tensor):
        return tensor.reshape((blocks, SPAN) + tensor.shape[1:])
    state_zero = jnp.zeros((RETENTION_HEADS, KEY_DIM, VALUE_DIM), jnp.float32)
    _, retained = lax.scan(block_step, state_zero, (split_blocks(rot_query), split_blocks(rot_key), split_blocks(value), split_blocks(log_decay)))
    retained = retained.reshape(FIRST_POSITIONS, RETENTION_HEADS, VALUE_DIM)
    average = lax.optimization_barrier(jnp.mean(retained, axis=-1, keepdims=True))
    centred = retained - average
    spread = lax.optimization_barrier(jnp.mean(centred * centred, axis=-1, keepdims=True))
    normed_heads = centred * lax.rsqrt(spread + EPSILON) * head_gain.reshape(RETENTION_HEADS, VALUE_DIM).astype(jnp.float32)
    gated = (jax.nn.silu(gate) * normed_heads.reshape(FIRST_POSITIONS, VALUE_WIDTH)).astype(jnp.bfloat16)
    group_cols = VALUE_WIDTH // N_TP
    summed = jnp.zeros((FIRST_POSITIONS, D), jnp.float32)
    for group in range(N_TP):
        lower = group * group_cols
        share_term = jnp.dot(gated[:, lower:lower + group_cols], output_weight[lower:lower + group_cols], preferred_element_type=jnp.float32).astype(jnp.bfloat16)
        summed = summed + share_term.astype(jnp.float32)
    return summed.astype(jnp.bfloat16)

def expert_mixture(expert_input, expert_gain, routes, group_weight, pair_weight, expert_gate, expert_up, expert_down):
    normed = layer_norm(expert_input, expert_gain).astype(jnp.bfloat16)
    flat_routes = routes.reshape(-1).astype(jnp.int32)
    capacity_rows = N_EP * N_TP * CAP
    mixing = (group_weight[:, None] * pair_weight).reshape(-1).astype(jnp.float32)

    def one_expert(carry, expert_id):
        matches = flat_routes == expert_id
        hits = jnp.nonzero(matches, size=capacity_rows, fill_value=0)[0].astype(jnp.int32)
        present = (jnp.arange(capacity_rows) < jnp.sum(matches)).astype(jnp.float32)
        token_ids = (hits // TOPK).astype(jnp.int32)
        gathered = normed[token_ids]
        gate_part = jnp.dot(gathered, expert_gate[expert_id], preferred_element_type=jnp.float32)
        up_part = jnp.dot(gathered, expert_up[expert_id], preferred_element_type=jnp.float32)
        hidden = (jax.nn.silu(gate_part) * up_part).astype(jnp.bfloat16)
        result = jnp.dot(hidden, expert_down[expert_id], preferred_element_type=jnp.float32).astype(jnp.bfloat16)
        contribution = result.astype(jnp.float32) * (mixing[hits] * present)[:, None]
        return (carry.at[token_ids].add(contribution), None)
    total, _ = lax.scan(one_expert, jnp.zeros((TOKENS_B, D), jnp.float32), jnp.arange(EXPERTS, dtype=jnp.int32))
    return total.astype(jnp.bfloat16)

def reference(mixer_input, log_decay, mixer_gain, query_weight, key_weight, value_weight, gate_weight, head_gain, output_weight, expert_input, expert_gain, routes, group_weight, pair_weight, expert_gate, expert_up, expert_down):
    mixer_output = token_mixer(mixer_input, log_decay, mixer_gain, query_weight, key_weight, value_weight, gate_weight, head_gain, output_weight)
    expert_output = expert_mixture(expert_input, expert_gain, routes, group_weight, pair_weight, expert_gate, expert_up, expert_down)
    return (mixer_output, expert_output)
```

```python
import functools
import math

import jax
import jax.numpy as jnp
import numpy as np
from jax import lax
from jax.experimental import pallas as pl
from jax.experimental.pallas import tpu as pltpu
from jax.sharding import PartitionSpec as P

KEY_DIM = 128
VALUE_DIM = 256
TOPK = 2
GROUPS = 4
LANES = 128
EPSILON = 1e-05
THETA = 10000.0
CHUNKS = 4
LOW = 64
MESH = pl.DeviceIdType.MESH
F32 = jnp.float32
BF16 = jnp.bfloat16


def ceil_to(value, unit):
    return -(-value // unit) * unit


def xor(index, mask):
    out = index
    bit = 1
    while bit <= mask:
        if mask & bit:
            out = out + bit * (1 - 2 * ((index // bit) % 2))
        bit *= 2
    return out


def dot(a, b):
    return jnp.dot(a, b, preferred_element_type=F32)


def rope_tables(length):
    half = KEY_DIM // 2
    frequency = THETA ** (-np.arange(half, dtype=np.float64) / half)
    frequency = np.concatenate([frequency, frequency])
    fine = np.arange(LOW)[:, None] * frequency
    coarse = (np.arange(length // LOW) * LOW)[:, None] * frequency
    return (
        np.stack([np.cos(coarse), np.sin(coarse)], axis=1).astype(np.float32),
        np.stack([np.cos(fine), np.sin(fine)], axis=0).astype(np.float32),
    )


def norm_rows(source, gain, store, rows, step=32):
    @pl.loop(0, rows // step)
    def _(i):
        at = pl.ds(pl.multiple_of(i * step, step), step)
        x = source[at, :].astype(F32)
        x = x - jnp.mean(x, axis=1, keepdims=True)
        spread = jnp.mean(x * x, axis=1, keepdims=True)
        store(at, (x * lax.rsqrt(spread + EPSILON) * gain[...]).astype(BF16))


def body(sizes, *refs):
    (ep_count, tp_count, cap) = sizes
    (
        xm_hbm, decay, mixer_gain, wq_hbm, wk_hbm, wv_hbm, wg_hbm, head_gain, wo_hbm,
        xe_hbm, expert_gain, routes, group_weight, pair_weight, eg_hbm, eu_hbm, ed_hbm,
        coarse, fine,
        mixer_out, expert_out,
        xm, xe, gathered, w_all, wo, eg, eu, ed, proj, cosine, sine, c_row, c_col,
        choose_t, spread_t, mixing, normed,
        packed, relayed, sent, arrived, acc, hidden, result, returned, combined, final,
        meta_out, meta_in,
        st_out, st_in, tot_out, tot_in, incoming,
        gated, terms, pair_in, far_out, far_in,
        load_sem, one_send, one_recv, z_send, z_recv, p_send, p_recv,
    ) = refs
    ep = lax.axis_index("ep")
    tp = lax.axis_index("tp")
    rows, width = xm.shape
    count = ep_count * tp_count
    plane = count // GROUPS
    cols = width // CHUNKS
    slots = packed.shape[2]
    block = sent.shape[2]
    keyw = wq_hbm.shape[1]
    valw = wv_hbm.shape[1]
    heads = keyw // KEY_DIM
    seg = rows * tp_count
    ff = eg.shape[1]
    me = ep * tp_count + tp
    my_plane = me // plane
    my_place = me % plane
    core = tp % 2
    pairs = tp_count // 2

    def at_flat(flat):
        return (flat // tp_count, flat % tp_count)

    def plane_peer(step):
        return at_flat((my_plane + step) % GROUPS * plane + my_place)

    def place_peer(place):
        return at_flat(my_plane * plane + place)

    strides = [1]
    if ep_count > 2:
        strides.append(2)
    covered = len(strides) if ep_count > 2 else 1
    while covered < ep_count - 1:
        strides.append(covered)
        covered *= 2

    loads = {}

    def load(name, source, target):
        copy = pltpu.make_async_copy(source, target, load_sem.at[len(loads)])
        copy.start()
        loads[name] = copy

    load("xm", xm_hbm, xm)
    load("xe", xe_hbm, xe)

    barrier = pltpu.get_barrier_semaphore()
    greeted = 0
    for step in range(1, GROUPS):
        pl.semaphore_signal(barrier, inc=1, device_id=plane_peer(step), device_id_type=MESH)
        greeted += 1
    for mask in range(1, plane):
        pl.semaphore_signal(
            barrier, inc=1, device_id=place_peer(xor(my_place, mask)), device_id_type=MESH
        )
        greeted += 1
    for stride in sorted(set(strides)):
        for other in ((ep + stride) % ep_count, (ep + ep_count - stride) % ep_count):
            pl.semaphore_signal(barrier, inc=1, device_id=(other, tp), device_id_type=MESH)
            greeted += 1

    loads["xm"].wait()
    load("wk", wk_hbm, w_all.at[:, pl.ds(0, keyw)])
    load("wv", wv_hbm, w_all.at[:, pl.ds(keyw, valw)])
    load("wq", wq_hbm, w_all.at[:, pl.ds(keyw + valw, keyw)])
    load("wg", wg_hbm, w_all.at[:, pl.ds(2 * keyw + valw, valw)])
    load("eg", eg_hbm.at[0], eg)
    load("eu", eu_hbm.at[0], eu)
    load("ed", ed_hbm.at[0], ed)
    load("wo", wo_hbm, wo)

    singles = []

    def send(source, target, device, when=None):
        index = len(singles)
        copy = pltpu.make_async_remote_copy(
            src_ref=source, dst_ref=target, send_sem=one_send.at[index],
            recv_sem=one_recv.at[index], device_id=device, device_id_type=MESH,
        )
        singles.append((copy, when))
        if when is None:
            copy.start()
        else:
            pl.when(when)(copy.start)
        return copy

    def keep_mixer(at, value):
        gathered[tp, at, :] = value

    norm_rows(xm, mixer_gain, keep_mixer, rows)
    pl.semaphore_wait(barrier, greeted)
    own = gathered.at[tp]
    far_arrivals = [
        send(own, own, {"tp": xor(tp, far)}) for far in range(2, tp_count, 2)
    ]
    near_arrival = send(own, own, {"tp": xor(tp, 1)})

    loads["xe"].wait()

    def keep_expert(at, value):
        normed[at, :] = value

    norm_rows(xe, expert_gain, keep_expert, rows)

    sub = lax.broadcasted_iota(jnp.int32, (rows, rows), 0)
    lane = lax.broadcasted_iota(jnp.int32, (rows, rows), 1)

    def stacked(lines):
        out = jnp.zeros((rows, rows), F32)
        for i, line in enumerate(lines):
            out = jnp.where(sub == i, line, out)
        return jnp.transpose(out)

    route = routes[...].astype(F32)
    picks = [route[k : k + 1, :] for k in range(TOPK)]
    columns = stacked(picks)
    pick_cols = [columns[:, k : k + 1] for k in range(TOPK)]
    earlier = sub < lane
    group = jnp.floor((picks[0] + 0.5) / plane)
    group_col = jnp.floor((pick_cols[0] + 0.5) / plane)

    def tally(hits):
        return jnp.sum(jnp.where(hits & earlier, 1.0, 0.0), axis=0, keepdims=True)

    place = group * slots + tally(group_col == group)
    lines = []
    for k in range(TOPK):
        hits = pick_cols[0] == picks[k]
        for other in range(1, TOPK):
            hits = hits | (pick_cols[other] == picks[k])
        lines.append((picks[k] - group * plane) * cap + tally(hits) + 1.0)
        lines.append(group_weight[...] * pair_weight[k : k + 1, :])
    lines.append(place)
    columns = stacked(lines)
    n_slots = GROUPS * slots
    choose = jnp.where(
        lax.broadcasted_iota(jnp.int32, (n_slots, rows), 0).astype(F32) == place, 1.0, 0.0
    ).astype(BF16)
    place_col = columns[:, 2 * TOPK : 2 * TOPK + 1]
    choose_t[...] = jnp.where(
        lax.broadcasted_iota(jnp.int32, (rows, n_slots), 1).astype(F32) == place_col, 1.0, 0.0
    ).astype(BF16)
    details = dot(choose, columns.astype(BF16)).astype(BF16)
    meta_out[...] = details.reshape(meta_out.shape)
    meta_in[my_plane] = meta_out[my_plane]
    steps = [2, 1, 3] if GROUPS == 4 else list(range(1, GROUPS))
    meta_arrivals = [
        send(
            meta_out.at[(my_plane + step) % GROUPS], meta_in.at[my_plane], plane_peer(step)
        )
        for step in steps
    ]

    def z_copies(phase, c, source, target):
        target[c, my_plane] = source[c, my_plane]
        for step in steps:
            pltpu.make_async_remote_copy(
                src_ref=source.at[c, (my_plane + step) % GROUPS],
                dst_ref=target.at[c, my_plane],
                send_sem=z_send.at[phase, c],
                recv_sem=z_recv.at[phase, c],
                device_id=plane_peer(step),
                device_id_type=MESH,
            ).start()

    def p_copies(phase, c, source, target):
        target[c, my_place] = source[c, my_place]
        for mask in range(plane - 1, 0, -1):
            other = xor(my_place, mask)
            pltpu.make_async_remote_copy(
                src_ref=source.at[c, other],
                dst_ref=target.at[c, my_place],
                send_sem=p_send.at[phase, c],
                recv_sem=p_recv.at[phase, c],
                device_id=place_peer(other),
                device_id_type=MESH,
            ).start()

    def wait_all(buffer, c, blocks, sem):
        part = buffer.at[c, pl.ds(0, blocks)]
        pltpu.make_async_copy(part, part, sem).wait()

    for c in range(CHUNKS):
        value = dot(choose, normed[:, c * cols : (c + 1) * cols]).astype(BF16)
        packed[c] = value.reshape(packed.shape[1:])
        z_copies(0, c, packed, relayed)

    sign = jnp.where(lax.broadcasted_iota(jnp.int32, (LOW, KEY_DIM), 1) < KEY_DIM // 2, -1.0, 1.0)

    @pl.loop(0, seg // LOW)
    def _(i):
        pair = coarse[ep * (seg // LOW) + i]
        at = pl.ds(pl.multiple_of(i * LOW, LOW), LOW)
        cosine[at, :] = pair[0:1] * fine[0] - pair[1:2] * fine[1]
        sine[at, :] = (pair[1:2] * fine[0] + pair[0:1] * fine[1]) * sign

    running = jnp.concatenate([decay[...], jnp.zeros((8 - heads, seg), F32)], axis=0)
    along = lax.broadcasted_iota(jnp.int32, running.shape, 1)
    shift = 1
    while shift < seg:
        running = running + jnp.where(along >= shift, pltpu.roll(running, shift, 1), 0.0)
        shift *= 2
    c_row[...] = running
    c_col[...] = jnp.transpose(running)

    for name in ("wk", "wv", "wq", "wg"):
        loads[name].wait()
    n_out = 2 * keyw + 2 * valw
    tile = 256 if n_out % 256 == 0 else 128

    def project(pair):
        at = pl.ds(pl.multiple_of(pair * 2 * rows, 2 * rows), 2 * rows)

        @pl.loop(0, n_out // tile)
        def _(n):
            part = pl.ds(pl.multiple_of(n * tile, tile), tile)
            lhs = gathered[pl.ds(pair * 2, 2)].reshape(2 * rows, width)
            proj[at, part] = dot(lhs, w_all[:, part]).astype(BF16)

    near_arrival.wait_recv()
    my_pair = tp // 2
    project(my_pair)

    for copy in meta_arrivals:
        copy.wait_recv()
    info = meta_in[...].reshape(n_slots, LANES).astype(F32)
    source = lax.broadcasted_iota(jnp.int32, (n_slots, 1), 0).astype(F32)
    source = jnp.floor((source + 0.5) / slots)
    n_pos = plane * block
    position = lax.broadcasted_iota(jnp.int32, (n_slots, n_pos), 1).astype(F32)
    spread = jnp.zeros((n_slots, n_pos), F32)
    shares = jnp.zeros((n_slots, n_pos), F32)
    for k in range(TOPK):
        target = info[:, 2 * k : 2 * k + 1] - 1.0
        expert = jnp.floor((target + 0.5) / cap)
        there = expert * block + source * cap + (target - expert * cap)
        there = jnp.where(target >= 0.0, there, -1.0)
        hit = position == there
        spread = jnp.where(hit, 1.0, spread)
        shares = jnp.where(hit, info[:, 2 * k + 1 : 2 * k + 2], shares)
    mixing[...] = shares.astype(BF16)
    full = ceil_to(n_slots, LANES)
    if full > n_slots:
        spread = jnp.concatenate([spread, jnp.zeros((full - n_slots, n_pos), F32)], axis=0)
    spread_t[...] = jnp.transpose(spread)[:, :n_slots].astype(BF16)

    def relay(c):
        wait_all(relayed, c, GROUPS - 1, z_recv.at[0, c])
        value = dot(spread_t[...], relayed[c].reshape(n_slots, cols)).astype(BF16)
        sent[c] = value.reshape(sent.shape[1:])
        p_copies(0, c, sent, arrived)

    half = CHUNKS // 2
    for c in range(half):
        relay(c)

    passed = []
    for place_in, far in enumerate(range(2, tp_count, 2)):
        far_arrivals[place_in].wait_recv()
        slot = gathered.at[xor(tp, far)]
        passed.append(send(slot, slot, {"tp": xor(tp, 1)}))
    for c in range(half, CHUNKS):
        relay(c)
    for place_in, far in enumerate(range(2, tp_count, 2)):
        passed[place_in].wait_recv()
        project(xor(my_pair, far // 2))

    def rotated(first):
        x = proj[:, first : first + KEY_DIM].astype(F32)
        return x * cosine[...] + pltpu.roll(x, KEY_DIM // 2, 1) * sine[...]

    for h in range(heads):
        key = rotated(h * KEY_DIM).astype(BF16)
        proj[:, h * KEY_DIM : (h + 1) * KEY_DIM] = key
        total = c_row[h : h + 1, seg - 1 : seg]
        remain = jnp.exp(total - c_col[:, h : h + 1])
        weighted = (key.astype(F32) * remain).astype(BF16)
        values = proj[:, keyw + h * VALUE_DIM : keyw + (h + 1) * VALUE_DIM]
        state = lax.dot_general(
            weighted, values, (((0,), (0,)), ((), ())), preferred_element_type=F32
        )
        st_out[0, h * KEY_DIM : (h + 1) * KEY_DIM, :] = state.astype(BF16)
    tot_out[0] = jnp.broadcast_to(c_row[:, seg - 1 : seg], tot_out.shape[1:])

    for i, stride in enumerate(strides):
        @pl.when(ep < stride)
        def _():
            st_in[i] = jnp.zeros(st_in.shape[1:], BF16)
            tot_in[i] = jnp.zeros(tot_in.shape[1:], F32)

    def state_send(slot, i):
        stride = strides[i]
        device = {"ep": (ep + stride) % ep_count}
        goes = ep + stride < ep_count
        return (
            send(tot_out.at[slot], tot_in.at[i], device, goes),
            send(st_out.at[slot], st_in.at[i], device, goes),
        )

    def state_recv(i, copies):
        @pl.when(ep >= strides[i])
        def _():
            for copy in copies:
                copy.wait_recv()

    def state_join(i):
        window = tot_in[0] if i == 1 else incoming_total[0]
        for h in range(heads):
            at = slice(h * KEY_DIM, (h + 1) * KEY_DIM)
            near = st_in[0, at, :].astype(F32) if i == 1 else incoming[at, :]
            scale = jnp.exp(window[h : h + 1, 0:1])
            incoming[at, :] = near + scale * st_in[i, at, :].astype(F32)
        incoming_total[0] = window + tot_in[i]

    incoming_total = [None]
    first_round = [state_send(0, i) for i in range(min(2, len(strides)))]

    loads["eg"].wait()
    loads["eu"].wait()
    ftile = 256

    def gate_up(c):
        wait_all(arrived, c, plane - 1, p_recv.at[0, c])
        deep = slice(c * cols, (c + 1) * cols)

        @pl.loop(0, ff // ftile)
        def _(n):
            part = pl.ds(pl.multiple_of(n * ftile, ftile), ftile)
            upper = pl.ds(pl.multiple_of(ff + n * ftile, ftile), ftile)
            lhs = arrived[c].reshape(n_pos, cols)
            gate = dot(lhs, eg[deep, part])
            up = dot(lhs, eu[deep, part])
            if c > 0:
                gate = gate + acc[:, part]
                up = up + acc[:, upper]
            if c < CHUNKS - 1:
                acc[:, part] = gate
                acc[:, upper] = up
            else:
                hidden[:, part] = (gate / (1.0 + jnp.exp(-gate)) * up).astype(BF16)

    def down(c):
        @pl.loop(0, cols // ftile)
        def _(n):
            part = pl.ds(pl.multiple_of(n * ftile, ftile), ftile)
            wide = pl.ds(pl.multiple_of(c * cols + n * ftile, ftile), ftile)
            value = dot(hidden[...], ed[:, wide]).astype(BF16)
            result[c, :, :, part] = value.reshape(plane, block, ftile)

        p_copies(1, c, result, returned)

    gate_up(0)
    gate_up(1)
    for i, copies in enumerate(first_round):
        state_recv(i, copies)
    if len(strides) > 1:
        state_join(1)
    else:
        incoming[...] = st_in[0].astype(F32)
        incoming_total[0] = tot_in[0]
    later = list(range(2, len(strides)))
    pending = None

    def next_state():
        i = later.pop(0)
        slot = i - 1
        st_out[slot] = incoming[...].astype(BF16)
        tot_out[slot] = incoming_total[0]
        return i, state_send(slot, i)

    def finish_state(waiting):
        i, copies = waiting
        state_recv(i, copies)
        state_join(i)

    if later:
        pending = next_state()
    for c in range(2, CHUNKS):
        gate_up(c)
    loads["ed"].wait()
    if pending:
        finish_state(pending)
        pending = next_state() if later else None
    for c in range(CHUNKS):
        down(c)
    while pending:
        finish_state(pending)
        pending = next_state() if later else None

    loads["wo"].wait()
    for h in range(heads):
        first = keyw + valw + h * KEY_DIM
        proj[:, first : first + KEY_DIM] = rotated(first).astype(BF16)

    def retention(pair):
        base = pair * 2 * rows

        @pl.loop(0, 2)
        def _(b):
            start = pl.multiple_of(base + b * rows, rows)
            at = pl.ds(start, rows)
            t = start + lax.broadcasted_iota(jnp.int32, (rows, seg), 0)
            s = lax.broadcasted_iota(jnp.int32, (rows, seg), 1)
            for h in range(heads):
                first = keyw + valw + h * KEY_DIM
                query = proj[at, first : first + KEY_DIM]
                key = proj[:, h * KEY_DIM : (h + 1) * KEY_DIM]
                values = proj[:, keyw + h * VALUE_DIM : keyw + (h + 1) * VALUE_DIM]
                column = c_col[at, h : h + 1]
                gaps = column - c_row[h : h + 1, :]
                weight = jnp.where(t >= s, jnp.exp(jnp.minimum(gaps, 0.0)), 0.0)
                scores = lax.dot_general(
                    query, key, (((1,), (1,)), ((), ())), preferred_element_type=F32
                )
                scaled = (query.astype(F32) * jnp.exp(column)).astype(BF16)
                before = incoming[h * KEY_DIM : (h + 1) * KEY_DIM, :].astype(BF16)
                x = dot((scores * weight).astype(BF16), values) + dot(scaled, before)
                x = x - jnp.mean(x, axis=1, keepdims=True)
                spread = jnp.mean(x * x, axis=1, keepdims=True)
                wide = slice(h * VALUE_DIM, (h + 1) * VALUE_DIM)
                x = x * lax.rsqrt(spread + EPSILON) * head_gain[:, wide]
                first = 2 * keyw + valw + h * VALUE_DIM
                gate = proj[at, first : first + VALUE_DIM].astype(F32)
                gated[at, wide] = (gate / (1.0 + jnp.exp(-gate)) * x).astype(BF16)

        at = pl.ds(pl.multiple_of(base, 2 * rows), 2 * rows)

        @pl.loop(0, width // ftile)
        def _(n):
            part = pl.ds(pl.multiple_of(n * ftile, ftile), ftile)
            value = dot(gated[at, :], wo[:, part]).astype(BF16)
            terms[pl.ds(pair * 2, 2), :, part] = value.reshape(2, rows, ftile)

    def add_rows(store, parts):
        @pl.loop(0, rows // 32)
        def _(i):
            at = pl.ds(pl.multiple_of(i * 32, 32), 32)
            total = parts[0](at).astype(F32)
            for part in parts[1:]:
                total = total + part(at).astype(F32)
            store(at, total.astype(BF16))

    def reduce_pair(i):
        pair = xor(my_pair, i)
        retention(pair)
        return send(terms.at[pair * 2 + 1 - core], pair_in.at[i], {"tp": xor(tp, 1)})

    from_core = {i: reduce_pair(i) for i in range(1, pairs)}
    from_far = []
    for i in range(1, pairs):
        from_core[i].wait_recv()
        mine = xor(my_pair, i) * 2 + core

        def keep_far(at, value, i=i):
            far_out[i - 1, at, :] = value

        add_rows(keep_far, [
            lambda at, mine=mine: terms[mine, at, :], lambda at, i=i: pair_in[i, at, :]
        ])
        from_far.append(send(far_out.at[i - 1], far_in.at[i - 1], {"tp": xor(tp, 2 * i)}))
    from_core[0] = reduce_pair(0)

    for c in range(CHUNKS):
        wait_all(returned, c, plane - 1, p_recv.at[1, c])
        value = dot(mixing[...], returned[c].reshape(n_pos, cols)).astype(BF16)
        combined[c] = value.reshape(combined.shape[1:])
        z_copies(1, c, combined, final)
    for c in range(CHUNKS):
        wait_all(final, c, GROUPS - 1, z_recv.at[1, c])
        value = dot(choose_t[...], final[c].reshape(n_slots, cols))
        expert_out[:, c * cols : (c + 1) * cols] = value.astype(BF16)

    from_core[0].wait_recv()
    for copy in from_far:
        copy.wait_recv()

    def keep_out(at, value):
        mixer_out[at, :] = value

    add_rows(keep_out, [
        lambda at: terms[tp, at, :], lambda at: pair_in[0, at, :]
    ] + [lambda at, i=i: far_in[i, at, :] for i in range(pairs - 1)])

    for copy, when in singles:
        if when is None:
            copy.wait_send()
        else:
            pl.when(when)(copy.wait_send)
    for c in range(CHUNKS):
        wait_all(packed, c, GROUPS - 1, z_send.at[0, c])
        wait_all(combined, c, GROUPS - 1, z_send.at[1, c])
        wait_all(sent, c, plane - 1, p_send.at[0, c])
        wait_all(result, c, plane - 1, p_send.at[1, c])


def local(
    ep_count, tp_count,
    mixer_input, log_decay, mixer_gain, query_weight, key_weight, value_weight, gate_weight,
    head_gain, output_weight, expert_input, expert_gain, routes, group_weight, pair_weight,
    expert_gate, expert_up, expert_down,
):
    rows, width = mixer_input.shape
    count = ep_count * tp_count
    plane = count // GROUPS
    cap = 3 * rows * TOPK // (2 * count)
    slots = ceil_to(plane * cap // TOPK, 16)
    block = ceil_to(cap * GROUPS, 16)
    cols = width // CHUNKS
    keyw = query_weight.shape[1]
    valw = value_weight.shape[1]
    heads = keyw // KEY_DIM
    seg = rows * tp_count
    ff = expert_gate.shape[2]
    n_slots = GROUPS * slots
    n_pos = plane * block
    pairs = tp_count // 2
    rounds = max(1, math.ceil(math.log2(ep_count))) + 1
    coarse, fine = rope_tables(seg * ep_count)

    def buf(*shape, dtype=BF16):
        return pltpu.VMEM(shape, dtype)

    dma = pltpu.SemaphoreType.DMA
    scratch = [
        buf(rows, width), buf(rows, width), buf(tp_count, rows, width),
        buf(width, 2 * keyw + 2 * valw), buf(valw, width),
        buf(width, ff), buf(width, ff), buf(ff, width),
        buf(seg, 2 * keyw + 2 * valw),
        buf(seg, KEY_DIM, dtype=F32), buf(seg, KEY_DIM, dtype=F32),
        buf(8, seg, dtype=F32), buf(seg, 8, dtype=F32),
        buf(rows, n_slots), buf(n_pos, n_slots), buf(n_slots, n_pos), buf(rows, width),
        buf(CHUNKS, GROUPS, slots, cols), buf(CHUNKS, GROUPS, slots, cols),
        buf(CHUNKS, plane, block, cols), buf(CHUNKS, plane, block, cols),
        buf(n_pos, 2 * ff, dtype=F32), buf(n_pos, ff),
        buf(CHUNKS, plane, block, cols), buf(CHUNKS, plane, block, cols),
        buf(CHUNKS, GROUPS, slots, cols), buf(CHUNKS, GROUPS, slots, cols),
        buf(GROUPS, slots, LANES), buf(GROUPS, slots, LANES),
        buf(rounds, keyw, VALUE_DIM), buf(rounds, keyw, VALUE_DIM),
        buf(rounds, 8, LANES, dtype=F32), buf(rounds, 8, LANES, dtype=F32),
        buf(keyw, VALUE_DIM, dtype=F32),
        buf(seg, valw), buf(tp_count, rows, width), buf(pairs, rows, width),
        buf(max(1, pairs - 1), rows, width), buf(max(1, pairs - 1), rows, width),
        dma((16,)), dma((32,)), dma((32,)),
        dma((2, CHUNKS)), dma((2, CHUNKS)), dma((2, CHUNKS)), dma((2, CHUNKS)),
    ]
    any_space = pl.BlockSpec(memory_space=pl.ANY)
    vmem = pl.BlockSpec(memory_space=pltpu.VMEM)
    shape = jax.ShapeDtypeStruct((rows, width), BF16)
    return pl.pallas_call(
        functools.partial(body, (ep_count, tp_count, cap)),
        out_shape=(shape, shape),
        in_specs=[
            any_space, vmem, vmem, any_space, any_space, any_space, any_space, vmem, any_space,
            any_space, vmem, vmem, vmem, vmem, any_space, any_space, any_space, vmem, vmem,
        ],
        out_specs=(vmem, vmem),
        scratch_shapes=scratch,
        compiler_params=pltpu.CompilerParams(
            collective_id=0, has_side_effects=True, vmem_limit_bytes=67_000_000
        ),
    )(
        mixer_input, log_decay.T, mixer_gain[None, :], query_weight, key_weight, value_weight,
        gate_weight, head_gain[None, :], output_weight, expert_input, expert_gain[None, :],
        routes.T, group_weight[None, :], pair_weight.T, expert_gate, expert_up, expert_down,
        jnp.asarray(coarse), jnp.asarray(fine),
    )


def solution(mesh):
    return jax.shard_map(
        functools.partial(local, mesh.shape["ep"], mesh.shape["tp"]),
        mesh=mesh,
        in_specs=(
            P(("ep", "tp"), None), P("ep", "tp"), P(), P(None, "tp"), P(None, "tp"),
            P(None, "tp"), P(None, "tp"), P("tp"), P("tp", None), P(("ep", "tp"), None), P(),
            P(("ep", "tp"), None), P(("ep", "tp")), P(("ep", "tp"), None),
            P(("ep", "tp"), None, None), P(("ep", "tp"), None, None),
            P(("ep", "tp"), None, None),
        ),
        out_specs=(P(("ep", "tp"), None), P(("ep", "tp"), None)),
        check_vma=False,
    )
```

```python
import functools

import jax
import jax.numpy as jnp
import numpy as np
from jax import lax
from jax.experimental import pallas as pl
from jax.experimental.pallas import tpu as pltpu
from jax.sharding import PartitionSpec as P

KEY_DIM = 128
VALUE_DIM = 256
TOPK = 2
GROUPS = 4
LANES = 128
EPSILON = 1e-05
THETA = 10000.0
CHUNKS = 8
VMEM_LIMIT = 60 * 2**20
DEEP = (2, 2, 2, 1, 1)
LOW = 64
MESH = pl.DeviceIdType.MESH
F32 = jnp.float32
BF16 = jnp.bfloat16

ORDER = (
    ("near_norm",), ("near_project",), ("spread_rows",), ("far_pass",), ("relay", 0), ("relay", 1), ("relay", 2), ("far_norm",), ("relay", 3), ("far_project",), ("states",), ("relay", 4), ("relay", 5), ("gate_up", 0), ("relay", 6), ("gate_up", 1), ("relay", 7), ("gate_up", 2), ("gate_up", 3), ("gate_up", 4), ("state_round", 0), ("down", 0), ("down", 1), ("down", 2), ("down", 3), ("down", 4), ("down", 5), ("down", 6), ("down", 7), ("queries",), ("combine", 0), ("state_round", 1), ("state_rest",), ("far_terms",), ("combine", 1), ("combine", 2), ("far_sums",), ("combine", 3), ("combine", 4), ("near_terms",), ("combine", 5), ("combine", 6), ("combine", 7), ("finish", 0), ("finish", 1), ("finish", 2), ("finish", 3), ("finish", 4), ("finish", 5), ("finish", 6), ("finish", 7), ("mixer_sum",),
)


def ceil_to(value, unit):
    return -(-value // unit) * unit


def xor(index, mask):
    out = index
    bit = 1
    while bit <= mask:
        if mask & bit:
            out = out + bit * (1 - 2 * ((index // bit) % 2))
        bit *= 2
    return out


def dot(a, b):
    return jnp.dot(a, b, preferred_element_type=F32)


def rope_tables(length):
    half = KEY_DIM // 2
    frequency = THETA ** (-np.arange(half, dtype=np.float64) / half)
    frequency = np.concatenate([frequency, frequency])
    fine = np.arange(LOW)[:, None] * frequency
    coarse = (np.arange(length // LOW) * LOW)[:, None] * frequency
    return (
        np.stack([np.cos(coarse), np.sin(coarse)], axis=1).astype(np.float32),
        np.stack([np.cos(fine), np.sin(fine)], axis=0).astype(np.float32),
    )


def state_strides(ep_count):
    rounds = []
    base = 1
    while base < ep_count:
        rounds.append([i * base for i in range(1, 4) if i * base < ep_count])
        base *= 4
    return rounds


def norm_rows(source, gain, store, rows, step=32):
    @pl.loop(0, rows // step)
    def _(i):
        at = pl.ds(pl.multiple_of(i * step, step), step)
        x = source[at, :].astype(F32)
        x = x - jnp.mean(x, axis=1, keepdims=True)
        spread = jnp.mean(x * x, axis=1, keepdims=True)
        store(at, (x * lax.rsqrt(spread + EPSILON) * gain[...]).astype(BF16))


def body(sizes, *refs):
    (ep_count, tp_count, cap) = sizes
    (
        xm_hbm, decay_hbm, mixer_gain_hbm, wq_hbm, wk_hbm, wv_hbm, wg_hbm, head_gain_hbm, wo_hbm,
        xe_hbm, expert_gain_hbm, routes_hbm, group_weight_hbm, pair_weight_hbm,
        eg_hbm, eu_hbm, ed_hbm, coarse_hbm, fine_hbm,
        mixer_out, expert_out,
        decay, mixer_gain, head_gain, xe, expert_gain, routes, group_weight, pair_weight,
        coarse, fine, gathered, mixer_rows, w_all, wo, eg, eu, ed, proj, cosine, sine, c_row, c_col,
        choose_t, spread_t, mixing, normed,
        packed, relayed, sent, arrived, acc, hidden, result, returned, combined, final,
        meta_out, meta_in,
        st_out, st_in, tot_out, tot_in, incoming, window_total,
        gated, terms, pair_in, far_out, far_in,
        load_sem, one_send, one_recv, z_send, z_recv, p_send, p_recv,
    ) = refs
    ep = lax.axis_index("ep")
    tp = lax.axis_index("tp")
    rows, width = xe.shape
    count = ep_count * tp_count
    plane = count // GROUPS
    cols = width // CHUNKS
    slots = packed.shape[2]
    block = sent.shape[2]
    keyw = wq_hbm.shape[1]
    valw = wv_hbm.shape[1]
    heads = keyw // KEY_DIM
    seg = rows * tp_count
    ff = eg.shape[1]
    me = ep * tp_count + tp
    my_plane = me // plane
    my_place = me % plane
    core = tp % 2
    pairs = tp_count // 2

    def at_flat(flat):
        return (flat // tp_count, flat % tp_count)

    def plane_peer(step):
        return at_flat((my_plane + step) % GROUPS * plane + my_place)

    def place_peer(place):
        return at_flat(my_plane * plane + place)

    rounds = state_strides(ep_count)
    strides = [stride for group in rounds for stride in group]

    loads = {}

    def load(name, source, target):
        copy = pltpu.make_async_copy(source, target, load_sem.at[len(loads)])
        copy.start()
        loads[name] = copy

    load("xe", xe_hbm, xe)
    load("routes", routes_hbm, routes)
    load("group_weight", group_weight_hbm, group_weight)
    load("pair_weight", pair_weight_hbm, pair_weight)
    load("expert_gain", expert_gain_hbm, expert_gain)
    small = list(loads)
    load("xm", xm_hbm, gathered.at[tp])
    load("mixer_gain", mixer_gain_hbm, mixer_gain)
    load("decay", decay_hbm, decay)
    load("head_gain", head_gain_hbm, head_gain)
    load("coarse", coarse_hbm.at[pl.ds(ep * coarse.shape[0], coarse.shape[0])], coarse)
    load("fine", fine_hbm, fine)
    others = [name for name in loads if name not in small]
    barrier = pltpu.get_barrier_semaphore()
    greeted = 0
    for step in range(1, GROUPS):
        pl.semaphore_signal(barrier, inc=1, device_id=plane_peer(step), device_id_type=MESH)
        greeted += 1
    for mask in range(1, plane):
        pl.semaphore_signal(
            barrier, inc=1, device_id=place_peer(xor(my_place, mask)), device_id_type=MESH
        )
        greeted += 1
    for stride in sorted(set(strides)):
        for other in ((ep + stride) % ep_count, (ep + ep_count - stride) % ep_count):
            pl.semaphore_signal(barrier, inc=1, device_id=(other, tp), device_id_type=MESH)
            greeted += 1

    singles = []

    def send(source, target, device, when=None):
        index = len(singles)
        copy = pltpu.make_async_remote_copy(
            src_ref=source, dst_ref=target, send_sem=one_send.at[index],
            recv_sem=one_recv.at[index], device_id=device, device_id_type=MESH,
        )
        singles.append((copy, when))
        if when is None:
            copy.start()
        else:
            pl.when(when)(copy.start)
        return copy

    pl.semaphore_wait(barrier, greeted)
    slot = gathered.at[tp]
    far_arrivals = [
        send(xm_hbm, slot, {"tp": xor(tp, far)}) for far in range(2, tp_count, 2)
    ]
    near_arrival = send(xm_hbm, slot, {"tp": xor(tp, 1)})
    load("wk", wk_hbm, w_all.at[:, pl.ds(0, keyw)])
    load("wv", wv_hbm, w_all.at[:, pl.ds(keyw, valw)])
    load("wq", wq_hbm, w_all.at[:, pl.ds(keyw + valw, keyw)])
    load("wg", wg_hbm, w_all.at[:, pl.ds(2 * keyw + valw, valw)])
    load("eg", eg_hbm.at[0], eg)
    load("eu", eu_hbm.at[0], eu)
    load("ed", ed_hbm.at[0], ed)
    load("wo", wo_hbm, wo)

    for name in small:
        loads[name].wait()

    def keep_expert(at, value):
        normed[at, :] = value

    norm_rows(xe, expert_gain, keep_expert, rows)

    sub = lax.broadcasted_iota(jnp.int32, (rows, rows), 0)
    lane = lax.broadcasted_iota(jnp.int32, (rows, rows), 1)

    def stacked(lines):
        out = jnp.zeros((rows, rows), F32)
        for i, line in enumerate(lines):
            out = jnp.where(sub == i, line, out)
        return jnp.transpose(out)

    route = routes[...].astype(F32)
    picks = [route[k : k + 1, :] for k in range(TOPK)]
    columns = stacked(picks)
    pick_cols = [columns[:, k : k + 1] for k in range(TOPK)]
    earlier = sub < lane
    group = jnp.floor((picks[0] + 0.5) / plane)
    group_col = jnp.floor((pick_cols[0] + 0.5) / plane)

    def tally(hits):
        return jnp.sum(jnp.where(hits & earlier, 1.0, 0.0), axis=0, keepdims=True)

    place = group * slots + tally(group_col == group)
    lines = []
    for k in range(TOPK):
        hits = pick_cols[0] == picks[k]
        for other in range(1, TOPK):
            hits = hits | (pick_cols[other] == picks[k])
        lines.append((picks[k] - group * plane) * cap + tally(hits) + 1.0)
        lines.append(group_weight[...] * pair_weight[k : k + 1, :])
    lines.append(place)
    columns = stacked(lines)
    n_slots = GROUPS * slots
    choose = jnp.where(
        lax.broadcasted_iota(jnp.int32, (n_slots, rows), 0).astype(F32) == place, 1.0, 0.0
    ).astype(BF16)
    place_col = columns[:, 2 * TOPK : 2 * TOPK + 1]
    choose_t[...] = jnp.where(
        lax.broadcasted_iota(jnp.int32, (rows, n_slots), 1).astype(F32) == place_col, 1.0, 0.0
    ).astype(BF16)
    details = dot(choose, columns.astype(BF16)).astype(BF16)
    meta_out[...] = details.reshape(meta_out.shape)
    meta_in[my_plane] = meta_out[my_plane]
    steps = [2, 1, 3] if GROUPS == 4 else list(range(1, GROUPS))
    meta_arrivals = [
        send(
            meta_out.at[(my_plane + step) % GROUPS], meta_in.at[my_plane], plane_peer(step)
        )
        for step in steps
    ]

    def z_copies(phase, c, source, target):
        target[c, my_plane] = source[c, my_plane]
        for step in steps:
            pltpu.make_async_remote_copy(
                src_ref=source.at[c, (my_plane + step) % GROUPS],
                dst_ref=target.at[c, my_plane],
                send_sem=z_send.at[phase, c],
                recv_sem=z_recv.at[phase, c],
                device_id=plane_peer(step),
                device_id_type=MESH,
            ).start()

    def p_copies(phase, c, source, target):
        target[c, my_place] = source[c, my_place]
        for mask in range(plane - 1, 0, -1):
            other = xor(my_place, mask)
            pltpu.make_async_remote_copy(
                src_ref=source.at[c, other],
                dst_ref=target.at[c, my_place],
                send_sem=p_send.at[phase, c],
                recv_sem=p_recv.at[phase, c],
                device_id=place_peer(other),
                device_id_type=MESH,
            ).start()

    def wait_all(buffer, c, blocks, sem):
        part = buffer.at[c, pl.ds(0, blocks)]
        pltpu.make_async_copy(part, part, sem).wait()

    for c in range(CHUNKS):
        value = dot(choose, normed[:, c * cols : (c + 1) * cols]).astype(BF16)
        packed[c] = value.reshape(packed.shape[1:])
        z_copies(0, c, packed, relayed)

    for name in others:
        loads[name].wait()
    sign = jnp.where(lax.broadcasted_iota(jnp.int32, (LOW, KEY_DIM), 1) < KEY_DIM // 2, -1.0, 1.0)

    @pl.loop(0, seg // LOW)
    def _(i):
        pair = coarse[i]
        at = pl.ds(pl.multiple_of(i * LOW, LOW), LOW)
        cosine[at, :] = pair[0:1] * fine[0] - pair[1:2] * fine[1]
        sine[at, :] = (pair[1:2] * fine[0] + pair[0:1] * fine[1]) * sign

    running = jnp.concatenate([decay[...], jnp.zeros((8 - heads, seg), F32)], axis=0)
    along = lax.broadcasted_iota(jnp.int32, running.shape, 1)
    shift = 1
    while shift < seg:
        running = running + jnp.where(along >= shift, pltpu.roll(running, shift, 1), 0.0)
        shift *= 2
    c_row[...] = running
    c_col[...] = jnp.transpose(running)

    n_out = 2 * keyw + 2 * valw
    tile = 256 if n_out % 256 == 0 else 128

    def weights():
        for name in ("wk", "wv", "wq", "wg"):
            loads[name].wait()

    def project(pair):
        at = pl.ds(pl.multiple_of(pair * 2 * rows, 2 * rows), 2 * rows)

        @pl.loop(0, n_out // tile)
        def _(n):
            part = pl.ds(pl.multiple_of(n * tile, tile), tile)
            lhs = mixer_rows[pl.ds(pair * 2, 2)].reshape(2 * rows, width)
            proj[at, part] = dot(lhs, w_all[:, part]).astype(BF16)

    order_of_steps = ORDER
    my_pair = tp // 2
    far_pairs = range(1, pairs)
    n_pos = plane * block
    ftile = 256

    def norm_block(place):
        def keep(at, value):
            mixer_rows[place, at, :] = value

        norm_rows(gathered.at[place], mixer_gain, keep, rows)

    def near_norm():
        norm_block(tp)
        near_arrival.wait_recv()
        norm_block(xor(tp, 1))

    def near_project():
        weights()
        project(my_pair)

    def spread_rows():
        for copy in meta_arrivals:
            copy.wait_recv()
        info = meta_in[...].reshape(n_slots, LANES).astype(F32)
        source = lax.broadcasted_iota(jnp.int32, (n_slots, 1), 0).astype(F32)
        source = jnp.floor((source + 0.5) / slots)
        position = lax.broadcasted_iota(jnp.int32, (n_slots, n_pos), 1).astype(F32)
        spread = jnp.zeros((n_slots, n_pos), F32)
        shares = jnp.zeros((n_slots, n_pos), F32)
        for k in range(TOPK):
            target = info[:, 2 * k : 2 * k + 1] - 1.0
            expert = jnp.floor((target + 0.5) / cap)
            there = expert * block + source * cap + (target - expert * cap)
            there = jnp.where(target >= 0.0, there, -1.0)
            hit = position == there
            spread = jnp.where(hit, 1.0, spread)
            shares = jnp.where(hit, info[:, 2 * k + 1 : 2 * k + 2], shares)
        mixing[...] = shares.astype(BF16)
        full = ceil_to(n_slots, LANES)
        if full > n_slots:
            spread = jnp.concatenate([spread, jnp.zeros((full - n_slots, n_pos), F32)], axis=0)
        spread_t[...] = jnp.transpose(spread)[:, :n_slots].astype(BF16)

    def relay(c):
        wait_all(relayed, c, GROUPS - 1, z_recv.at[0, c])
        value = dot(spread_t[...], relayed[c].reshape(n_slots, cols)).astype(BF16)
        sent[c] = value.reshape(sent.shape[1:])
        p_copies(0, c, sent, arrived)

    passed = []

    def far_pass():
        for i in far_pairs:
            far_arrivals[i - 1].wait_recv()
            slot = gathered.at[xor(tp, 2 * i)]
            passed.append(send(slot, slot, {"tp": xor(tp, 1)}))

    def far_norm():
        for i in far_pairs:
            norm_block(xor(tp, 2 * i))
            passed[i - 1].wait_recv()
            norm_block(xor(tp, 2 * i + 1))

    def far_project():
        for i in far_pairs:
            project(xor(my_pair, i))

    def rotated(first):
        x = proj[:, first : first + KEY_DIM].astype(F32)
        return x * cosine[...] + pltpu.roll(x, KEY_DIM // 2, 1) * sine[...]

    prefix = {}

    def state_send(r):
        for stride in rounds[r]:
            i = strides.index(stride)
            device = {"ep": (ep + stride) % ep_count}
            goes = ep + stride < ep_count
            prefix[i] = (
                send(tot_out.at[r], tot_in.at[i], device, goes),
                send(st_out.at[r], st_in.at[i], device, goes),
            )

    def states():
        for h in range(heads):
            key = rotated(h * KEY_DIM).astype(BF16)
            proj[:, h * KEY_DIM : (h + 1) * KEY_DIM] = key
            total = c_row[h : h + 1, seg - 1 : seg]
            remain = jnp.exp(total - c_col[:, h : h + 1])
            weighted = (key.astype(F32) * remain).astype(BF16)
            values = proj[:, keyw + h * VALUE_DIM : keyw + (h + 1) * VALUE_DIM]
            state = lax.dot_general(
                weighted, values, (((0,), (0,)), ((), ())), preferred_element_type=F32
            )
            st_out[0, h * KEY_DIM : (h + 1) * KEY_DIM, :] = state.astype(BF16)
        tot_out[0] = jnp.broadcast_to(c_row[:, seg - 1 : seg], tot_out.shape[1:])
        for i, stride in enumerate(strides):
            @pl.when(ep < stride)
            def _():
                st_in[i] = jnp.zeros(st_in.shape[1:], BF16)
                tot_in[i] = jnp.zeros(tot_in.shape[1:], F32)
        state_send(0)

    def state_recv(i):
        @pl.when(ep >= strides[i])
        def _():
            for copy in prefix[i]:
                copy.wait_recv()

    def state_round(r):
        if r >= len(rounds):
            return
        for stride in rounds[r]:
            i = strides.index(stride)
            state_recv(i)
            for h in range(heads):
                at = slice(h * KEY_DIM, (h + 1) * KEY_DIM)
                part = st_in[i, at, :].astype(F32)
                if i > 0:
                    scale = jnp.exp(window_total[h : h + 1, 0:1])
                    part = incoming[at, :] + scale * part
                incoming[at, :] = part
            window_total[...] = tot_in[i] + (window_total[...] if i > 0 else 0.0)
        if r + 1 < len(rounds):
            for h in range(heads):
                at = slice(h * KEY_DIM, (h + 1) * KEY_DIM)
                scale = jnp.exp(tot_out[0, h : h + 1, 0:1])
                whole = st_out[0, at, :].astype(F32) + scale * incoming[at, :]
                st_out[r + 1, at, :] = whole.astype(BF16)
            tot_out[r + 1] = tot_out[0] + window_total[...]
            state_send(r + 1)

    def state_rest():
        for r in range(2, len(rounds)):
            state_round(r)

    def gate_up(c):
        if c == 0:
            loads["eg"].wait()
            loads["eu"].wait()
        group = range(sum(DEEP[:c]), sum(DEEP[: c + 1]))
        for i in group:
            wait_all(arrived, i, plane - 1, p_recv.at[0, i])

        @pl.loop(0, ff // ftile)
        def _(n):
            part = pl.ds(pl.multiple_of(n * ftile, ftile), ftile)
            upper = pl.ds(pl.multiple_of(ff + n * ftile, ftile), ftile)
            gate = acc[:, part] if c > 0 else 0.0
            up = acc[:, upper] if c > 0 else 0.0
            for i in group:
                lhs = arrived[i].reshape(n_pos, cols)
                deep = slice(i * cols, (i + 1) * cols)
                gate = gate + dot(lhs, eg[deep, part])
                up = up + dot(lhs, eu[deep, part])
            if c < len(DEEP) - 1:
                acc[:, part] = gate
                acc[:, upper] = up
            else:
                hidden[:, part] = (gate / (1.0 + jnp.exp(-gate)) * up).astype(BF16)

    def down(c):
        if c == 0:
            loads["ed"].wait()

        @pl.loop(0, cols // ftile)
        def _(n):
            part = pl.ds(pl.multiple_of(n * ftile, ftile), ftile)
            wide = pl.ds(pl.multiple_of(c * cols + n * ftile, ftile), ftile)
            value = dot(hidden[...], ed[:, wide]).astype(BF16)
            result[c, :, :, part] = value.reshape(plane, block, ftile)

        p_copies(1, c, result, returned)

    def queries():
        loads["wo"].wait()
        for h in range(heads):
            first = keyw + valw + h * KEY_DIM
            proj[:, first : first + KEY_DIM] = rotated(first).astype(BF16)

    def retention(pair):
        base = pair * 2 * rows

        @pl.loop(0, 2)
        def _(b):
            start = pl.multiple_of(base + b * rows, rows)
            at = pl.ds(start, rows)
            t = start + lax.broadcasted_iota(jnp.int32, (rows, seg), 0)
            s = lax.broadcasted_iota(jnp.int32, (rows, seg), 1)
            for h in range(heads):
                first = keyw + valw + h * KEY_DIM
                query = proj[at, first : first + KEY_DIM]
                key = proj[:, h * KEY_DIM : (h + 1) * KEY_DIM]
                values = proj[:, keyw + h * VALUE_DIM : keyw + (h + 1) * VALUE_DIM]
                column = c_col[at, h : h + 1]
                gaps = column - c_row[h : h + 1, :]
                weight = jnp.where(t >= s, jnp.exp(jnp.minimum(gaps, 0.0)), 0.0)
                scores = lax.dot_general(
                    query, key, (((1,), (1,)), ((), ())), preferred_element_type=F32
                )
                scaled = (query.astype(F32) * jnp.exp(column)).astype(BF16)
                before = incoming[h * KEY_DIM : (h + 1) * KEY_DIM, :].astype(BF16)
                x = dot((scores * weight).astype(BF16), values) + dot(scaled, before)
                x = x - jnp.mean(x, axis=1, keepdims=True)
                spread = jnp.mean(x * x, axis=1, keepdims=True)
                wide = slice(h * VALUE_DIM, (h + 1) * VALUE_DIM)
                x = x * lax.rsqrt(spread + EPSILON) * head_gain[:, wide]
                first = 2 * keyw + valw + h * VALUE_DIM
                gate = proj[at, first : first + VALUE_DIM].astype(F32)
                gated[at, wide] = (gate / (1.0 + jnp.exp(-gate)) * x).astype(BF16)

        at = pl.ds(pl.multiple_of(base, 2 * rows), 2 * rows)

        @pl.loop(0, width // ftile)
        def _(n):
            part = pl.ds(pl.multiple_of(n * ftile, ftile), ftile)
            value = dot(gated[at, :], wo[:, part]).astype(BF16)
            terms[pl.ds(pair * 2, 2), :, part] = value.reshape(2, rows, ftile)

    def add_rows(store, parts):
        @pl.loop(0, rows // 32)
        def _(i):
            at = pl.ds(pl.multiple_of(i * 32, 32), 32)
            total = parts[0](at).astype(F32)
            for part in parts[1:]:
                total = total + part(at).astype(F32)
            store(at, total.astype(BF16))

    from_core = {}
    from_far = []

    def reduce_pair(i):
        pair = xor(my_pair, i)
        retention(pair)
        from_core[i] = send(terms.at[pair * 2 + 1 - core], pair_in.at[i], {"tp": xor(tp, 1)})

    def far_terms():
        for i in far_pairs:
            reduce_pair(i)

    def far_sums():
        for i in far_pairs:
            from_core[i].wait_recv()
            mine = xor(my_pair, i) * 2 + core

            def keep_far(at, value, i=i):
                far_out[i - 1, at, :] = value

            add_rows(keep_far, [
                lambda at, mine=mine: terms[mine, at, :], lambda at, i=i: pair_in[i, at, :]
            ])
            from_far.append(send(far_out.at[i - 1], far_in.at[i - 1], {"tp": xor(tp, 2 * i)}))

    def near_terms():
        reduce_pair(0)

    def combine(c):
        wait_all(returned, c, plane - 1, p_recv.at[1, c])
        value = dot(mixing[...], returned[c].reshape(n_pos, cols)).astype(BF16)
        combined[c] = value.reshape(combined.shape[1:])
        z_copies(1, c, combined, final)

    def finish(c):
        wait_all(final, c, GROUPS - 1, z_recv.at[1, c])
        value = dot(choose_t[...], final[c].reshape(n_slots, cols))
        expert_out[:, c * cols : (c + 1) * cols] = value.astype(BF16)

    def mixer_sum():
        from_core[0].wait_recv()
        for copy in from_far:
            copy.wait_recv()

        def keep_out(at, value):
            mixer_out[at, :] = value

        add_rows(keep_out, [
            lambda at: terms[tp, at, :], lambda at: pair_in[0, at, :]
        ] + [lambda at, i=i: far_in[i, at, :] for i in range(pairs - 1)])

    steps_by_name = locals()
    for name, *args in order_of_steps:
        steps_by_name[name](*args)

    for copy, when in singles:
        if when is None:
            copy.wait_send()
        else:
            pl.when(when)(copy.wait_send)
    for c in range(CHUNKS):
        wait_all(packed, c, GROUPS - 1, z_send.at[0, c])
        wait_all(combined, c, GROUPS - 1, z_send.at[1, c])
        wait_all(sent, c, plane - 1, p_send.at[0, c])
        wait_all(result, c, plane - 1, p_send.at[1, c])


def hand_out(mixed_in, expert_in, mixed_out, expert_out, sem):
    copies = [
        pltpu.make_async_copy(mixed_in, mixed_out, sem.at[0]),
        pltpu.make_async_copy(expert_in, expert_out, sem.at[1]),
    ]
    for copy in copies:
        copy.start()
    for copy in copies:
        copy.wait()


def local(
    ep_count, tp_count,
    mixer_input, log_decay, mixer_gain, query_weight, key_weight, value_weight, gate_weight,
    head_gain, output_weight, expert_input, expert_gain, routes, group_weight, pair_weight,
    expert_gate, expert_up, expert_down,
):
    rows, width = mixer_input.shape
    count = ep_count * tp_count
    plane = count // GROUPS
    cap = 3 * rows * TOPK // (2 * count)
    slots = ceil_to(plane * cap // TOPK, 16)
    block = ceil_to(cap * GROUPS, 16)
    cols = width // CHUNKS
    keyw = query_weight.shape[1]
    valw = value_weight.shape[1]
    heads = keyw // KEY_DIM
    seg = rows * tp_count
    ff = expert_gate.shape[2]
    n_slots = GROUPS * slots
    n_pos = plane * block
    pairs = tp_count // 2
    rounds = len(state_strides(ep_count))
    distances = sum(len(group) for group in state_strides(ep_count))
    coarse, fine = rope_tables(seg * ep_count)

    def buf(*shape, dtype=BF16):
        return pltpu.VMEM(shape, dtype)

    dma = pltpu.SemaphoreType.DMA
    scratch = [
        buf(heads, seg, dtype=F32), buf(1, width, dtype=F32), buf(1, valw, dtype=F32),
        buf(rows, width), buf(1, width, dtype=F32), buf(TOPK, rows, dtype=jnp.int32),
        buf(1, rows, dtype=F32), buf(TOPK, rows, dtype=F32),
        buf(seg // LOW, 2, KEY_DIM, dtype=F32), buf(2, LOW, KEY_DIM, dtype=F32),
        buf(tp_count, rows, width), buf(tp_count, rows, width),
        buf(width, 2 * keyw + 2 * valw), buf(valw, width),
        buf(width, ff), buf(width, ff), buf(ff, width),
        buf(seg, 2 * keyw + 2 * valw),
        buf(seg, KEY_DIM, dtype=F32), buf(seg, KEY_DIM, dtype=F32),
        buf(8, seg, dtype=F32), buf(seg, 8, dtype=F32),
        buf(rows, n_slots), buf(n_pos, n_slots), buf(n_slots, n_pos), buf(rows, width),
        buf(CHUNKS, GROUPS, slots, cols), buf(CHUNKS, GROUPS, slots, cols),
        buf(CHUNKS, plane, block, cols), buf(CHUNKS, plane, block, cols),
        buf(n_pos, 2 * ff, dtype=F32), buf(n_pos, ff),
        buf(CHUNKS, plane, block, cols), buf(CHUNKS, plane, block, cols),
        buf(CHUNKS, GROUPS, slots, cols), buf(CHUNKS, GROUPS, slots, cols),
        buf(GROUPS, slots, LANES), buf(GROUPS, slots, LANES),
        buf(rounds, keyw, VALUE_DIM), buf(distances, keyw, VALUE_DIM),
        buf(rounds, 8, LANES, dtype=F32), buf(distances, 8, LANES, dtype=F32),
        buf(keyw, VALUE_DIM, dtype=F32), buf(8, LANES, dtype=F32),
        buf(seg, valw), buf(tp_count, rows, width), buf(pairs, rows, width),
        buf(max(1, pairs - 1), rows, width), buf(max(1, pairs - 1), rows, width),
        dma((20,)), dma((32,)), dma((32,)),
        dma((2, CHUNKS)), dma((2, CHUNKS)), dma((2, CHUNKS)), dma((2, CHUNKS)),
    ]
    any_space = pl.BlockSpec(memory_space=pl.ANY)
    vmem = pl.BlockSpec(memory_space=pltpu.VMEM)
    shape = jax.ShapeDtypeStruct((rows, width), BF16)
    outs = pl.pallas_call(
        functools.partial(body, (ep_count, tp_count, cap)),
        out_shape=(buf(rows, width), buf(rows, width)),
        in_specs=[any_space] * 19,
        out_specs=(vmem, vmem),
        scratch_shapes=scratch,
        compiler_params=pltpu.CompilerParams(
            collective_id=0, has_side_effects=True, vmem_limit_bytes=VMEM_LIMIT
        ),
    )(
        mixer_input, log_decay.T, mixer_gain[None, :], query_weight, key_weight, value_weight,
        gate_weight, head_gain[None, :], output_weight, expert_input, expert_gain[None, :],
        routes.T, group_weight[None, :], pair_weight.T, expert_gate, expert_up, expert_down,
        jnp.asarray(coarse), jnp.asarray(fine),
    )
    outs = [pltpu.with_memory_space_constraint(out, pltpu.VMEM) for out in outs]
    return pl.pallas_call(
        hand_out,
        out_shape=(shape, shape),
        in_specs=[vmem, vmem],
        out_specs=(any_space, any_space),
        scratch_shapes=[dma((2,))],
    )(*outs)


def solution(mesh):
    return jax.shard_map(
        functools.partial(local, mesh.shape["ep"], mesh.shape["tp"]),
        mesh=mesh,
        in_specs=(
            P(("ep", "tp"), None), P("ep", "tp"), P(), P(None, "tp"), P(None, "tp"),
            P(None, "tp"), P(None, "tp"), P("tp"), P("tp", None), P(("ep", "tp"), None), P(),
            P(("ep", "tp"), None), P(("ep", "tp")), P(("ep", "tp"), None),
            P(("ep", "tp"), None, None), P(("ep", "tp"), None, None),
            P(("ep", "tp"), None, None),
        ),
        out_specs=(P(("ep", "tp"), None), P(("ep", "tp"), None)),
        check_vma=False,
    )
```

```python
import functools

import jax
import jax.numpy as jnp
import numpy as np
from jax import lax
from jax.experimental import pallas as pl
from jax.experimental.pallas import tpu as pltpu
from jax.sharding import PartitionSpec as P

KEY_DIM = 128
VALUE_DIM = 256
TOPK = 2
GROUPS = 4
LANES = 128
EPSILON = 1e-05
THETA = 10000.0
CHUNKS = 8
VMEM_LIMIT = 60 * 2**20
DEEP = (2, 2, 2, 1, 1)
LOW = 64
MESH = pl.DeviceIdType.MESH
F32 = jnp.float32
BF16 = jnp.bfloat16

ORDER = (
    ("near_norm",), ("spread_rows",), ("relay", 0), ("near_project",), ("relay", 1), ("far_pass",), ("relay_far", 0), ("relay_far", 1), ("relay", 2), ("relay_far", 2), ("far_norm",), ("relay", 3), ("relay_far", 3), ("far_project",), ("relay", 4), ("relay_far", 4), ("states",), ("relay", 5), ("relay_far", 5), ("gate_up", 0), ("relay", 6), ("relay_far", 6), ("relay", 7), ("relay_far", 7), ("state_send",), ("gate_up", 1), ("gate_up", 2), ("gate_up", 3), ("gate_up", 4), ("state_plane",), ("down", 0), ("down", 1), ("down", 2), ("down", 3), ("down", 4), ("state_hop", 0), ("down", 5), ("down", 6), ("down", 7), ("queries",), ("combine", 0), ("combine", 1), ("state_hop", 1), ("far_terms",), ("combine", 2), ("far_sums",), ("combine", 3), ("combine", 4), ("combine", 5), ("combine", 6), ("combine", 7), ("near_terms",), ("finish", 0), ("finish", 1), ("finish", 2), ("finish", 3), ("finish", 4), ("finish", 5), ("finish", 6), ("finish", 7), ("mixer_sum",),
)


def ceil_to(value, unit):
    return -(-value // unit) * unit


def xor(index, mask):
    out = index
    bit = 1
    while bit <= mask:
        if mask & bit:
            out = out + bit * (1 - 2 * ((index // bit) % 2))
        bit *= 2
    return out


def dot(a, b):
    return jnp.dot(a, b, preferred_element_type=F32)


def rope_tables(length):
    half = KEY_DIM // 2
    frequency = THETA ** (-np.arange(half, dtype=np.float64) / half)
    frequency = np.concatenate([frequency, frequency])
    fine = np.arange(LOW)[:, None] * frequency
    coarse = (np.arange(length // LOW) * LOW)[:, None] * frequency
    return (
        np.stack([np.cos(coarse), np.sin(coarse)], axis=1).astype(np.float32),
        np.stack([np.cos(fine), np.sin(fine)], axis=0).astype(np.float32),
    )


def norm_rows(source, gain, store, rows, step=32):
    @pl.loop(0, rows // step)
    def _(i):
        at = pl.ds(pl.multiple_of(i * step, step), step)
        x = source[at, :].astype(F32)
        x = x - jnp.mean(x, axis=1, keepdims=True)
        spread = jnp.mean(x * x, axis=1, keepdims=True)
        store(at, (x * lax.rsqrt(spread + EPSILON) * gain[...]).astype(BF16))


def body(sizes, *refs):
    (ep_count, tp_count, cap) = sizes
    (
        xm_hbm, decay_hbm, mixer_gain_hbm, wq_hbm, wk_hbm, wv_hbm, wg_hbm, head_gain_hbm, wo_hbm,
        xe_hbm, expert_gain_hbm, routes_hbm, group_weight_hbm, pair_weight_hbm,
        eg_hbm, eu_hbm, ed_hbm, coarse_hbm, fine_hbm,
        mixer_out, expert_out,
        decay, mixer_gain, head_gain, xe, expert_gain, routes, group_weight, pair_weight,
        coarse, fine, gathered, mixer_rows, w_all, wo, eg, eu, ed, proj, cosine, sine, c_row, c_col,
        choose_t, spread_t, mixing, normed,
        packed, relayed, sent, arrived, acc, hidden, result, returned, combined, final,
        meta_out, meta_in,
        st_out, st_in, tot_out, tot_in, incoming, whole, window_total,
        gated, terms, pair_in, far_out, far_in,
        load_sem, one_send, one_recv, z_send, z_recv, p_send, p_recv,
    ) = refs
    ep = lax.axis_index("ep")
    tp = lax.axis_index("tp")
    rows, width = xe.shape
    count = ep_count * tp_count
    plane = count // GROUPS
    cols = width // CHUNKS
    slots = packed.shape[2]
    block = sent.shape[2]
    keyw = wq_hbm.shape[1]
    valw = wv_hbm.shape[1]
    heads = keyw // KEY_DIM
    seg = rows * tp_count
    ff = eg.shape[1]
    me = ep * tp_count + tp
    my_plane = me // plane
    my_place = me % plane
    core = tp % 2
    pairs = tp_count // 2

    def at_flat(flat):
        return (flat // tp_count, flat % tp_count)

    def plane_peer(step):
        return at_flat((my_plane + step) % GROUPS * plane + my_place)

    def place_peer(place):
        return at_flat(my_plane * plane + place)

    inner = ep_count // GROUPS
    inside = ep % inner
    hops = [1 << b for b in range((GROUPS - 1).bit_length())]

    loads = {}

    def load(name, source, target):
        copy = pltpu.make_async_copy(source, target, load_sem.at[len(loads)])
        copy.start()
        loads[name] = copy

    load("xe", xe_hbm, xe)
    load("routes", routes_hbm, routes)
    load("group_weight", group_weight_hbm, group_weight)
    load("pair_weight", pair_weight_hbm, pair_weight)
    load("expert_gain", expert_gain_hbm, expert_gain)
    small = list(loads)
    load("xm", xm_hbm, gathered.at[tp])
    load("mixer_gain", mixer_gain_hbm, mixer_gain)
    load("decay", decay_hbm, decay)
    load("head_gain", head_gain_hbm, head_gain)
    load("coarse", coarse_hbm.at[pl.ds(ep * coarse.shape[0], coarse.shape[0])], coarse)
    load("fine", fine_hbm, fine)
    others = [name for name in loads if name not in small]
    barrier = pltpu.get_barrier_semaphore()
    greeted = 0
    for step in range(1, GROUPS):
        pl.semaphore_signal(barrier, inc=1, device_id=plane_peer(step), device_id_type=MESH)
        greeted += 1
    for mask in range(1, plane):
        pl.semaphore_signal(
            barrier, inc=1, device_id=place_peer(xor(my_place, mask)), device_id_type=MESH
        )
        greeted += 1
    singles = []

    def send(source, target, device, when=None):
        index = len(singles)
        copy = pltpu.make_async_remote_copy(
            src_ref=source, dst_ref=target, send_sem=one_send.at[index],
            recv_sem=one_recv.at[index], device_id=device, device_id_type=MESH,
        )
        singles.append((copy, when))
        if when is None:
            copy.start()
        else:
            pl.when(when)(copy.start)
        return copy

    pl.semaphore_wait(barrier, greeted)
    slot = gathered.at[tp]
    far_arrivals = [
        send(xm_hbm, slot, {"tp": xor(tp, far)}) for far in range(2, tp_count, 2)
    ]
    near_arrival = send(xm_hbm, slot, {"tp": xor(tp, 1)})
    load("wk", wk_hbm, w_all.at[:, pl.ds(0, keyw)])
    load("wv", wv_hbm, w_all.at[:, pl.ds(keyw, valw)])
    load("wq", wq_hbm, w_all.at[:, pl.ds(keyw + valw, keyw)])
    load("wg", wg_hbm, w_all.at[:, pl.ds(2 * keyw + valw, valw)])
    load("eg", eg_hbm.at[0], eg)
    load("eu", eu_hbm.at[0], eu)
    load("ed", ed_hbm.at[0], ed)
    load("wo", wo_hbm, wo)

    for name in small:
        loads[name].wait()

    def keep_expert(at, value):
        normed[at, :] = value

    norm_rows(xe, expert_gain, keep_expert, rows)

    sub = lax.broadcasted_iota(jnp.int32, (rows, rows), 0)
    lane = lax.broadcasted_iota(jnp.int32, (rows, rows), 1)

    def stacked(lines):
        out = jnp.zeros((rows, rows), F32)
        for i, line in enumerate(lines):
            out = jnp.where(sub == i, line, out)
        return jnp.transpose(out)

    route = routes[...].astype(F32)
    picks = [route[k : k + 1, :] for k in range(TOPK)]
    columns = stacked(picks)
    pick_cols = [columns[:, k : k + 1] for k in range(TOPK)]
    earlier = sub < lane
    group = jnp.floor((picks[0] + 0.5) / plane)
    group_col = jnp.floor((pick_cols[0] + 0.5) / plane)

    def tally(hits):
        return jnp.sum(jnp.where(hits & earlier, 1.0, 0.0), axis=0, keepdims=True)

    place = group * slots + tally(group_col == group)
    lines = []
    for k in range(TOPK):
        hits = pick_cols[0] == picks[k]
        for other in range(1, TOPK):
            hits = hits | (pick_cols[other] == picks[k])
        lines.append((picks[k] - group * plane) * cap + tally(hits) + 1.0)
        lines.append(group_weight[...] * pair_weight[k : k + 1, :])
    lines.append(place)
    columns = stacked(lines)
    n_slots = GROUPS * slots
    choose = jnp.where(
        lax.broadcasted_iota(jnp.int32, (n_slots, rows), 0).astype(F32) == place, 1.0, 0.0
    ).astype(BF16)
    place_col = columns[:, 2 * TOPK : 2 * TOPK + 1]
    choose_t[...] = jnp.where(
        lax.broadcasted_iota(jnp.int32, (rows, n_slots), 1).astype(F32) == place_col, 1.0, 0.0
    ).astype(BF16)
    details = dot(choose, columns.astype(BF16)).astype(BF16)
    meta_out[...] = details.reshape(meta_out.shape)
    meta_in[my_plane] = meta_out[my_plane]
    steps = [2, 1, 3] if GROUPS == 4 else list(range(1, GROUPS))
    meta_arrivals = [
        send(
            meta_out.at[(my_plane + step) % GROUPS], meta_in.at[my_plane], plane_peer(step)
        )
        for step in steps
    ]

    def z_copies(phase, c, source, target):
        target[c, my_plane] = source[c, my_plane]
        for step in steps:
            pltpu.make_async_remote_copy(
                src_ref=source.at[c, (my_plane + step) % GROUPS],
                dst_ref=target.at[c, my_plane],
                send_sem=z_send.at[phase, c],
                recv_sem=z_recv.at[phase, c],
                device_id=plane_peer(step),
                device_id_type=MESH,
            ).start()

    masks = range(plane - 1, 0, -1)
    across = [mask for mask in masks if mask % tp_count > 1]
    aside = [mask for mask in masks if mask % tp_count <= 1]

    def p_copies(phase, c, source, target, masks):
        for mask in masks:
            other = xor(my_place, mask)
            pltpu.make_async_remote_copy(
                src_ref=source.at[c, other],
                dst_ref=target.at[c, my_place],
                send_sem=p_send.at[phase, c],
                recv_sem=p_recv.at[phase, c],
                device_id=place_peer(other),
                device_id_type=MESH,
            ).start()

    def wait_all(buffer, c, blocks, sem):
        part = buffer.at[c, pl.ds(0, blocks)]
        pltpu.make_async_copy(part, part, sem).wait()

    for c in range(CHUNKS):
        value = dot(choose, normed[:, c * cols : (c + 1) * cols]).astype(BF16)
        packed[c] = value.reshape(packed.shape[1:])
        z_copies(0, c, packed, relayed)

    for name in others:
        loads[name].wait()
    sign = jnp.where(lax.broadcasted_iota(jnp.int32, (LOW, KEY_DIM), 1) < KEY_DIM // 2, -1.0, 1.0)

    @pl.loop(0, seg // LOW)
    def _(i):
        pair = coarse[i]
        at = pl.ds(pl.multiple_of(i * LOW, LOW), LOW)
        cosine[at, :] = pair[0:1] * fine[0] - pair[1:2] * fine[1]
        sine[at, :] = (pair[1:2] * fine[0] + pair[0:1] * fine[1]) * sign

    running = jnp.concatenate([decay[...], jnp.zeros((8 - heads, seg), F32)], axis=0)
    along = lax.broadcasted_iota(jnp.int32, running.shape, 1)
    shift = 1
    while shift < seg:
        running = running + jnp.where(along >= shift, pltpu.roll(running, shift, 1), 0.0)
        shift *= 2
    c_row[...] = running
    c_col[...] = jnp.transpose(running)

    n_out = 2 * keyw + 2 * valw
    tile = 256 if n_out % 256 == 0 else 128

    def weights():
        for name in ("wk", "wv", "wq", "wg"):
            loads[name].wait()

    def project(pair):
        at = pl.ds(pl.multiple_of(pair * 2 * rows, 2 * rows), 2 * rows)

        @pl.loop(0, n_out // tile)
        def _(n):
            part = pl.ds(pl.multiple_of(n * tile, tile), tile)
            lhs = mixer_rows[pl.ds(pair * 2, 2)].reshape(2 * rows, width)
            proj[at, part] = dot(lhs, w_all[:, part]).astype(BF16)

    order_of_steps = ORDER
    my_pair = tp // 2
    far_pairs = range(1, pairs)
    n_pos = plane * block
    ftile = 256

    def norm_block(place):
        def keep(at, value):
            mixer_rows[place, at, :] = value

        norm_rows(gathered.at[place], mixer_gain, keep, rows)

    def near_norm():
        norm_block(tp)
        near_arrival.wait_recv()
        norm_block(xor(tp, 1))

    def near_project():
        weights()
        project(my_pair)

    def spread_rows():
        for copy in meta_arrivals:
            copy.wait_recv()
        info = meta_in[...].reshape(n_slots, LANES).astype(F32)
        source = lax.broadcasted_iota(jnp.int32, (n_slots, 1), 0).astype(F32)
        source = jnp.floor((source + 0.5) / slots)
        position = lax.broadcasted_iota(jnp.int32, (n_slots, n_pos), 1).astype(F32)
        spread = jnp.zeros((n_slots, n_pos), F32)
        shares = jnp.zeros((n_slots, n_pos), F32)
        for k in range(TOPK):
            target = info[:, 2 * k : 2 * k + 1] - 1.0
            expert = jnp.floor((target + 0.5) / cap)
            there = expert * block + source * cap + (target - expert * cap)
            there = jnp.where(target >= 0.0, there, -1.0)
            hit = position == there
            spread = jnp.where(hit, 1.0, spread)
            shares = jnp.where(hit, info[:, 2 * k + 1 : 2 * k + 2], shares)
        mixing[...] = shares.astype(BF16)
        full = ceil_to(n_slots, LANES)
        if full > n_slots:
            spread = jnp.concatenate([spread, jnp.zeros((full - n_slots, n_pos), F32)], axis=0)
        spread_t[...] = jnp.transpose(spread)[:, :n_slots].astype(BF16)

    def relay(c):
        wait_all(relayed, c, GROUPS - 1, z_recv.at[0, c])
        value = dot(spread_t[...], relayed[c].reshape(n_slots, cols)).astype(BF16)
        sent[c] = value.reshape(sent.shape[1:])
        p_copies(0, c, sent, arrived, aside)
        arrived[c, my_place] = sent[c, my_place]

    def relay_far(c):
        p_copies(0, c, sent, arrived, across)

    passed = []

    def far_pass():
        for i in far_pairs:
            far_arrivals[i - 1].wait_recv()
            slot = gathered.at[xor(tp, 2 * i)]
            passed.append(send(slot, slot, {"tp": xor(tp, 1)}))

    def far_norm():
        for i in far_pairs:
            norm_block(xor(tp, 2 * i))
            passed[i - 1].wait_recv()
            norm_block(xor(tp, 2 * i + 1))

    def far_project():
        for i in far_pairs:
            project(xor(my_pair, i))

    def rotated(first):
        x = proj[:, first : first + KEY_DIM].astype(F32)
        return x * cosine[...] + pltpu.roll(x, KEY_DIM // 2, 1) * sine[...]

    def states():
        for h in range(heads):
            key = rotated(h * KEY_DIM).astype(BF16)
            proj[:, h * KEY_DIM : (h + 1) * KEY_DIM] = key
            total = c_row[h : h + 1, seg - 1 : seg]
            remain = jnp.exp(total - c_col[:, h : h + 1])
            weighted = (key.astype(F32) * remain).astype(BF16)
            values = proj[:, keyw + h * VALUE_DIM : keyw + (h + 1) * VALUE_DIM]
            state = lax.dot_general(
                weighted, values, (((0,), (0,)), ((), ())), preferred_element_type=F32
            )
            st_out[0, h * KEY_DIM : (h + 1) * KEY_DIM, :] = state.astype(BF16)
        tot_out[0] = jnp.broadcast_to(c_row[:, seg - 1 : seg], tot_out.shape[1:])
        st_in[inside] = st_out[0]
        tot_in[inside] = tot_out[0]
        for b, hop in enumerate(hops):
            @pl.when(my_plane < hop)
            def _():
                st_in[inner + b] = jnp.zeros(st_in.shape[1:], BF16)
                tot_in[inner + b] = jnp.zeros(tot_in.shape[1:], F32)

    arrivals = {}

    def state_send():
        arrivals[0] = []
        for j in range(1, inner):
            device = {"ep": my_plane * inner + (inside + j) % inner}
            arrivals[0].append(send(tot_out.at[0], tot_in.at[inside], device))
            arrivals[0].append(send(st_out.at[0], st_in.at[inside], device))

    def plane_send(b):
        if b < len(hops):
            device = {"ep": (ep + hops[b] * inner) % ep_count}
            goes = my_plane + hops[b] < GROUPS
            st_out[b + 1] = whole[...].astype(BF16)
            arrivals[b + 1] = [
                send(tot_out.at[b + 1], tot_in.at[inner + b], device, goes),
                send(st_out.at[b + 1], st_in.at[inner + b], device, goes),
            ]

    def state_plane():
        for copy in arrivals[0]:
            copy.wait_recv()
        total = tot_in[0]
        window = jnp.where(inside > 0, total, 0.0)
        for h in range(heads):
            at = slice(h * KEY_DIM, (h + 1) * KEY_DIM)
            part = st_in[0, at, :].astype(F32)
            whole[at, :] = part
            incoming[at, :] = jnp.where(inside > 0, part, 0.0)
        for i in range(1, inner):
            for h in range(heads):
                at = slice(h * KEY_DIM, (h + 1) * KEY_DIM)
                part = st_in[i, at, :].astype(F32)
                scale = jnp.exp(tot_in[i, h : h + 1, 0:1])
                whole[at, :] = part + scale * whole[at, :]
                if i < inner - 1:
                    joined = part + scale * incoming[at, :]
                    incoming[at, :] = jnp.where(inside > i, joined, incoming[at, :])
            total = total + tot_in[i]
            window = jnp.where(inside > i, window + tot_in[i], window)
        window_total[...] = window
        tot_out[1] = total
        plane_send(0)

    def state_hop(b):
        @pl.when(my_plane >= hops[b])
        def _():
            for copy in arrivals[b + 1]:
                copy.wait_recv()

        for h in range(heads):
            at = slice(h * KEY_DIM, (h + 1) * KEY_DIM)
            part = st_in[inner + b, at, :].astype(F32)
            incoming[at, :] = incoming[at, :] + jnp.exp(window_total[h : h + 1, 0:1]) * part
            if b + 1 < len(hops):
                scale = jnp.exp(tot_out[b + 1, h : h + 1, 0:1])
                whole[at, :] = whole[at, :] + scale * part
        window_total[...] = window_total[...] + tot_in[inner + b]
        if b + 1 < len(hops):
            tot_out[b + 2] = tot_out[b + 1] + tot_in[inner + b]
            plane_send(b + 1)

    def gate_up(c):
        if c == 0:
            loads["eg"].wait()
            loads["eu"].wait()
        group = range(sum(DEEP[:c]), sum(DEEP[: c + 1]))
        for i in group:
            wait_all(arrived, i, plane - 1, p_recv.at[0, i])

        @pl.loop(0, ff // ftile)
        def _(n):
            part = pl.ds(pl.multiple_of(n * ftile, ftile), ftile)
            upper = pl.ds(pl.multiple_of(ff + n * ftile, ftile), ftile)
            gate = acc[:, part] if c > 0 else 0.0
            up = acc[:, upper] if c > 0 else 0.0
            for i in group:
                lhs = arrived[i].reshape(n_pos, cols)
                deep = slice(i * cols, (i + 1) * cols)
                gate = gate + dot(lhs, eg[deep, part])
                up = up + dot(lhs, eu[deep, part])
            if c < len(DEEP) - 1:
                acc[:, part] = gate
                acc[:, upper] = up
            else:
                hidden[:, part] = (gate / (1.0 + jnp.exp(-gate)) * up).astype(BF16)

    def down(c):
        if c == 0:
            loads["ed"].wait()

        @pl.loop(0, cols // ftile)
        def _(n):
            part = pl.ds(pl.multiple_of(n * ftile, ftile), ftile)
            wide = pl.ds(pl.multiple_of(c * cols + n * ftile, ftile), ftile)
            value = dot(hidden[...], ed[:, wide]).astype(BF16)
            result[c, :, :, part] = value.reshape(plane, block, ftile)

        p_copies(1, c, result, returned, masks)
        returned[c, my_place] = result[c, my_place]

    def queries():
        loads["wo"].wait()
        for h in range(heads):
            first = keyw + valw + h * KEY_DIM
            proj[:, first : first + KEY_DIM] = rotated(first).astype(BF16)

    def retention(pair):
        base = pair * 2 * rows

        @pl.loop(0, 2)
        def _(b):
            start = pl.multiple_of(base + b * rows, rows)
            at = pl.ds(start, rows)
            t = start + lax.broadcasted_iota(jnp.int32, (rows, seg), 0)
            s = lax.broadcasted_iota(jnp.int32, (rows, seg), 1)
            for h in range(heads):
                first = keyw + valw + h * KEY_DIM
                query = proj[at, first : first + KEY_DIM]
                key = proj[:, h * KEY_DIM : (h + 1) * KEY_DIM]
                values = proj[:, keyw + h * VALUE_DIM : keyw + (h + 1) * VALUE_DIM]
                column = c_col[at, h : h + 1]
                gaps = column - c_row[h : h + 1, :]
                weight = jnp.where(t >= s, jnp.exp(jnp.minimum(gaps, 0.0)), 0.0)
                scores = lax.dot_general(
                    query, key, (((1,), (1,)), ((), ())), preferred_element_type=F32
                )
                scaled = (query.astype(F32) * jnp.exp(column)).astype(BF16)
                before = incoming[h * KEY_DIM : (h + 1) * KEY_DIM, :].astype(BF16)
                x = dot((scores * weight).astype(BF16), values) + dot(scaled, before)
                x = x - jnp.mean(x, axis=1, keepdims=True)
                spread = jnp.mean(x * x, axis=1, keepdims=True)
                wide = slice(h * VALUE_DIM, (h + 1) * VALUE_DIM)
                x = x * lax.rsqrt(spread + EPSILON) * head_gain[:, wide]
                first = 2 * keyw + valw + h * VALUE_DIM
                gate = proj[at, first : first + VALUE_DIM].astype(F32)
                gated[at, wide] = (gate / (1.0 + jnp.exp(-gate)) * x).astype(BF16)

        at = pl.ds(pl.multiple_of(base, 2 * rows), 2 * rows)

        @pl.loop(0, width // ftile)
        def _(n):
            part = pl.ds(pl.multiple_of(n * ftile, ftile), ftile)
            value = dot(gated[at, :], wo[:, part]).astype(BF16)
            terms[pl.ds(pair * 2, 2), :, part] = value.reshape(2, rows, ftile)

    def add_rows(store, parts):
        @pl.loop(0, rows // 32)
        def _(i):
            at = pl.ds(pl.multiple_of(i * 32, 32), 32)
            total = parts[0](at).astype(F32)
            for part in parts[1:]:
                total = total + part(at).astype(F32)
            store(at, total.astype(BF16))

    from_core = {}
    from_far = []

    def reduce_pair(i):
        pair = xor(my_pair, i)
        retention(pair)
        from_core[i] = send(terms.at[pair * 2 + 1 - core], pair_in.at[i], {"tp": xor(tp, 1)})

    def far_terms():
        for i in far_pairs:
            reduce_pair(i)

    def far_sums():
        for i in far_pairs:
            from_core[i].wait_recv()
            mine = xor(my_pair, i) * 2 + core

            def keep_far(at, value, i=i):
                far_out[i - 1, at, :] = value

            add_rows(keep_far, [
                lambda at, mine=mine: terms[mine, at, :], lambda at, i=i: pair_in[i, at, :]
            ])
            from_far.append(send(far_out.at[i - 1], far_in.at[i - 1], {"tp": xor(tp, 2 * i)}))

    def near_terms():
        reduce_pair(0)

    def combine(c):
        wait_all(returned, c, plane - 1, p_recv.at[1, c])
        value = dot(mixing[...], returned[c].reshape(n_pos, cols)).astype(BF16)
        combined[c] = value.reshape(combined.shape[1:])
        z_copies(1, c, combined, final)

    def finish(c):
        wait_all(final, c, GROUPS - 1, z_recv.at[1, c])
        value = dot(choose_t[...], final[c].reshape(n_slots, cols))
        expert_out[:, c * cols : (c + 1) * cols] = value.astype(BF16)

    def mixer_sum():
        from_core[0].wait_recv()
        for copy in from_far:
            copy.wait_recv()

        def keep_out(at, value):
            mixer_out[at, :] = value

        add_rows(keep_out, [
            lambda at: terms[tp, at, :], lambda at: pair_in[0, at, :]
        ] + [lambda at, i=i: far_in[i, at, :] for i in range(pairs - 1)])

    steps_by_name = locals()
    for name, *args in order_of_steps:
        steps_by_name[name](*args)

    for copy, when in singles:
        if when is None:
            copy.wait_send()
        else:
            pl.when(when)(copy.wait_send)
    for c in range(CHUNKS):
        wait_all(packed, c, GROUPS - 1, z_send.at[0, c])
        wait_all(combined, c, GROUPS - 1, z_send.at[1, c])
        wait_all(sent, c, plane - 1, p_send.at[0, c])
        wait_all(result, c, plane - 1, p_send.at[1, c])


def hand_out(mixed_in, expert_in, mixed_out, expert_out, sem):
    copies = [
        pltpu.make_async_copy(mixed_in, mixed_out, sem.at[0]),
        pltpu.make_async_copy(expert_in, expert_out, sem.at[1]),
    ]
    for copy in copies:
        copy.start()
    for copy in copies:
        copy.wait()


def local(
    ep_count, tp_count,
    mixer_input, log_decay, mixer_gain, query_weight, key_weight, value_weight, gate_weight,
    head_gain, output_weight, expert_input, expert_gain, routes, group_weight, pair_weight,
    expert_gate, expert_up, expert_down,
):
    rows, width = mixer_input.shape
    count = ep_count * tp_count
    plane = count // GROUPS
    cap = 3 * rows * TOPK // (2 * count)
    slots = ceil_to(plane * cap // TOPK, 16)
    block = ceil_to(cap * GROUPS, 16)
    cols = width // CHUNKS
    keyw = query_weight.shape[1]
    valw = value_weight.shape[1]
    heads = keyw // KEY_DIM
    seg = rows * tp_count
    ff = expert_gate.shape[2]
    n_slots = GROUPS * slots
    n_pos = plane * block
    pairs = tp_count // 2
    hops = (GROUPS - 1).bit_length()
    rounds = hops + 1
    distances = ep_count // GROUPS + hops
    coarse, fine = rope_tables(seg * ep_count)

    def buf(*shape, dtype=BF16):
        return pltpu.VMEM(shape, dtype)

    dma = pltpu.SemaphoreType.DMA
    scratch = [
        buf(heads, seg, dtype=F32), buf(1, width, dtype=F32), buf(1, valw, dtype=F32),
        buf(rows, width), buf(1, width, dtype=F32), buf(TOPK, rows, dtype=jnp.int32),
        buf(1, rows, dtype=F32), buf(TOPK, rows, dtype=F32),
        buf(seg // LOW, 2, KEY_DIM, dtype=F32), buf(2, LOW, KEY_DIM, dtype=F32),
        buf(tp_count, rows, width), buf(tp_count, rows, width),
        buf(width, 2 * keyw + 2 * valw), buf(valw, width),
        buf(width, ff), buf(width, ff), buf(ff, width),
        buf(seg, 2 * keyw + 2 * valw),
        buf(seg, KEY_DIM, dtype=F32), buf(seg, KEY_DIM, dtype=F32),
        buf(8, seg, dtype=F32), buf(seg, 8, dtype=F32),
        buf(rows, n_slots), buf(n_pos, n_slots), buf(n_slots, n_pos), buf(rows, width),
        buf(CHUNKS, GROUPS, slots, cols), buf(CHUNKS, GROUPS, slots, cols),
        buf(CHUNKS, plane, block, cols), buf(CHUNKS, plane, block, cols),
        buf(n_pos, 2 * ff, dtype=F32), buf(n_pos, ff),
        buf(CHUNKS, plane, block, cols), buf(CHUNKS, plane, block, cols),
        buf(CHUNKS, GROUPS, slots, cols), buf(CHUNKS, GROUPS, slots, cols),
        buf(GROUPS, slots, LANES), buf(GROUPS, slots, LANES),
        buf(rounds, keyw, VALUE_DIM), buf(distances, keyw, VALUE_DIM),
        buf(rounds, 8, LANES, dtype=F32), buf(distances, 8, LANES, dtype=F32),
        buf(keyw, VALUE_DIM, dtype=F32), buf(keyw, VALUE_DIM, dtype=F32), buf(8, LANES, dtype=F32),
        buf(seg, valw), buf(tp_count, rows, width), buf(pairs, rows, width),
        buf(max(1, pairs - 1), rows, width), buf(max(1, pairs - 1), rows, width),
        dma((20,)), dma((32,)), dma((32,)),
        dma((2, CHUNKS)), dma((2, CHUNKS)), dma((2, CHUNKS)), dma((2, CHUNKS)),
    ]
    any_space = pl.BlockSpec(memory_space=pl.ANY)
    vmem = pl.BlockSpec(memory_space=pltpu.VMEM)
    shape = jax.ShapeDtypeStruct((rows, width), BF16)
    outs = pl.pallas_call(
        functools.partial(body, (ep_count, tp_count, cap)),
        out_shape=(buf(rows, width), buf(rows, width)),
        in_specs=[any_space] * 19,
        out_specs=(vmem, vmem),
        scratch_shapes=scratch,
        compiler_params=pltpu.CompilerParams(
            collective_id=0, has_side_effects=True, vmem_limit_bytes=VMEM_LIMIT
        ),
    )(
        mixer_input, log_decay.T, mixer_gain[None, :], query_weight, key_weight, value_weight,
        gate_weight, head_gain[None, :], output_weight, expert_input, expert_gain[None, :],
        routes.T, group_weight[None, :], pair_weight.T, expert_gate, expert_up, expert_down,
        jnp.asarray(coarse), jnp.asarray(fine),
    )
    outs = [pltpu.with_memory_space_constraint(out, pltpu.VMEM) for out in outs]
    return pl.pallas_call(
        hand_out,
        out_shape=(shape, shape),
        in_specs=[vmem, vmem],
        out_specs=(any_space, any_space),
        scratch_shapes=[dma((2,))],
    )(*outs)


def solution(mesh):
    return jax.shard_map(
        functools.partial(local, mesh.shape["ep"], mesh.shape["tp"]),
        mesh=mesh,
        in_specs=(
            P(("ep", "tp"), None), P("ep", "tp"), P(), P(None, "tp"), P(None, "tp"),
            P(None, "tp"), P(None, "tp"), P("tp"), P("tp", None), P(("ep", "tp"), None), P(),
            P(("ep", "tp"), None), P(("ep", "tp")), P(("ep", "tp"), None),
            P(("ep", "tp"), None, None), P(("ep", "tp"), None, None),
            P(("ep", "tp"), None, None),
        ),
        out_specs=(P(("ep", "tp"), None), P(("ep", "tp"), None)),
        check_vma=False,
    )
```

```python
import functools

import jax
import jax.numpy as jnp
import numpy as np
from jax import lax
from jax.experimental import pallas as pl
from jax.experimental.pallas import tpu as pltpu
from jax.sharding import PartitionSpec as P

KEY_DIM = 128
VALUE_DIM = 256
TOPK = 2
GROUPS = 4
LANES = 128
EPSILON = 1e-05
THETA = 10000.0
CHUNKS = 8
VMEM_LIMIT = 60 * 2**20
DEEP = (2, 2, 2, 1, 1)
LOW = 64
MESH = pl.DeviceIdType.MESH
F32 = jnp.float32
BF16 = jnp.bfloat16

ORDER = (
    ("near_norm",), ("spread_rows",), ("relay", 0), ("near_project",), ("relay", 1),
    ("far_pass",), ("relay_far", 0), ("relay_far", 1), ("relay", 2), ("relay_far", 2),
    ("far_norm",), ("relay", 3), ("relay_far", 3), ("far_project",), ("relay", 4),
    ("relay_far", 4), ("states",), ("relay", 5), ("relay_far", 5), ("gate_up", 0), ("relay", 6),
    ("relay_far", 6), ("relay", 7), ("relay_far", 7), ("state_send",), ("gate_up", 1),
    ("gate_up", 2), ("gate_up", 3), ("gate_up", 4), ("down", 0), ("state_plane",), ("down", 1),
    ("down", 2), ("down", 3), ("down", 4), ("down", 5), ("state_hop", 0), ("down", 6),
    ("down", 7), ("queries",), ("combine", 0), ("combine", 1), ("combine", 2), ("state_hop", 1),
    ("far_terms",), ("combine", 3), ("combine", 4), ("far_sums",), ("combine", 5), ("combine", 6),
    ("combine", 7), ("near_terms",), ("finish", 0), ("finish", 1), ("finish", 2), ("finish", 3),
    ("finish", 4), ("finish", 5), ("finish", 6), ("finish", 7), ("mixer_sum",),
)


def ceil_to(value, unit):
    return -(-value // unit) * unit


def xor(index, mask):
    out = index
    bit = 1
    while bit <= mask:
        if mask & bit:
            out = out + bit * (1 - 2 * ((index // bit) % 2))
        bit *= 2
    return out


def dot(a, b):
    return jnp.dot(a, b, preferred_element_type=F32)


def rope_tables(length):
    half = KEY_DIM // 2
    frequency = THETA ** (-np.arange(half, dtype=np.float64) / half)
    frequency = np.concatenate([frequency, frequency])
    fine = np.arange(LOW)[:, None] * frequency
    coarse = (np.arange(length // LOW) * LOW)[:, None] * frequency
    return (
        np.stack([np.cos(coarse), np.sin(coarse)], axis=1).astype(np.float32),
        np.stack([np.cos(fine), np.sin(fine)], axis=0).astype(np.float32),
    )


def norm_rows(source, gain, store, rows, step=32):
    @pl.loop(0, rows // step)
    def _(i):
        at = pl.ds(pl.multiple_of(i * step, step), step)
        x = source[at, :].astype(F32)
        x = x - jnp.mean(x, axis=1, keepdims=True)
        spread = jnp.mean(x * x, axis=1, keepdims=True)
        store(at, (x * lax.rsqrt(spread + EPSILON) * gain[...]).astype(BF16))


def body(sizes, *refs):
    (ep_count, tp_count, cap) = sizes
    (
        xm_hbm, decay_hbm, mixer_gain_hbm, wq_hbm, wk_hbm, wv_hbm, wg_hbm, head_gain_hbm, wo_hbm,
        xe_hbm, expert_gain_hbm, routes_hbm, group_weight_hbm, pair_weight_hbm,
        eg_hbm, eu_hbm, ed_hbm, coarse_hbm, fine_hbm,
        mixer_out, expert_out,
        decay, mixer_gain, head_gain, xe, expert_gain, routes, group_weight, pair_weight,
        coarse, fine, gathered, mixer_rows, w_all, wo, eg, eu, ed, proj, cosine, sine, c_row, c_col,
        choose_t, spread_t, mixing, normed,
        packed, relayed, sent, arrived, acc, hidden, result, returned, combined, final,
        meta_out, meta_in,
        st_out, st_in, tot_out, tot_in, incoming, whole, window_total,
        gated, terms, pair_in, far_out, far_in,
        load_sem, one_send, one_recv, z_send, z_recv, p_send, p_recv,
    ) = refs
    ep = lax.axis_index("ep")
    tp = lax.axis_index("tp")
    rows, width = xe.shape
    count = ep_count * tp_count
    plane = count // GROUPS
    cols = width // CHUNKS
    slots = packed.shape[2]
    block = sent.shape[2]
    keyw = wq_hbm.shape[1]
    valw = wv_hbm.shape[1]
    heads = keyw // KEY_DIM
    seg = rows * tp_count
    ff = eg.shape[1]
    me = ep * tp_count + tp
    my_plane = me // plane
    my_place = me % plane
    core = tp % 2
    pairs = tp_count // 2

    def at_flat(flat):
        return (flat // tp_count, flat % tp_count)

    def plane_peer(step):
        return at_flat((my_plane + step) % GROUPS * plane + my_place)

    def place_peer(place):
        return at_flat(my_plane * plane + place)

    inner = ep_count // GROUPS
    inside = ep % inner
    hops = [1 << b for b in range((GROUPS - 1).bit_length())]

    loads = {}

    def load(name, source, target):
        copy = pltpu.make_async_copy(source, target, load_sem.at[len(loads)])
        copy.start()
        loads[name] = copy

    load("xe", xe_hbm, xe)
    load("routes", routes_hbm, routes)
    load("group_weight", group_weight_hbm, group_weight)
    load("pair_weight", pair_weight_hbm, pair_weight)
    load("expert_gain", expert_gain_hbm, expert_gain)
    small = list(loads)
    load("xm", xm_hbm, gathered.at[tp])
    load("mixer_gain", mixer_gain_hbm, mixer_gain)
    load("decay", decay_hbm, decay)
    load("head_gain", head_gain_hbm, head_gain)
    load("coarse", coarse_hbm.at[pl.ds(ep * coarse.shape[0], coarse.shape[0])], coarse)
    load("fine", fine_hbm, fine)
    others = [name for name in loads if name not in small]
    barrier = pltpu.get_barrier_semaphore()
    greeted = 0
    for step in range(1, GROUPS):
        pl.semaphore_signal(barrier, inc=1, device_id=plane_peer(step), device_id_type=MESH)
        greeted += 1
    for mask in range(1, plane):
        pl.semaphore_signal(
            barrier, inc=1, device_id=place_peer(xor(my_place, mask)), device_id_type=MESH
        )
        greeted += 1
    singles = []

    def send(source, target, device, when=None):
        index = len(singles)
        copy = pltpu.make_async_remote_copy(
            src_ref=source, dst_ref=target, send_sem=one_send.at[index],
            recv_sem=one_recv.at[index], device_id=device, device_id_type=MESH,
        )
        singles.append((copy, when))
        if when is None:
            copy.start()
        else:
            pl.when(when)(copy.start)
        return copy

    pl.semaphore_wait(barrier, greeted)
    slot = gathered.at[tp]
    far_arrivals = [
        send(xm_hbm, slot, {"tp": xor(tp, far)}) for far in range(2, tp_count, 2)
    ]
    near_arrival = send(xm_hbm, slot, {"tp": xor(tp, 1)})
    load("wk", wk_hbm, w_all.at[:, pl.ds(0, keyw)])
    load("wv", wv_hbm, w_all.at[:, pl.ds(keyw, valw)])
    load("wq", wq_hbm, w_all.at[:, pl.ds(keyw + valw, keyw)])
    load("wg", wg_hbm, w_all.at[:, pl.ds(2 * keyw + valw, valw)])
    load("eg", eg_hbm.at[0], eg)
    load("eu", eu_hbm.at[0], eu)
    load("ed", ed_hbm.at[0], ed)
    load("wo", wo_hbm, wo)

    for name in small:
        loads[name].wait()

    def keep_expert(at, value):
        normed[at, :] = value

    norm_rows(xe, expert_gain, keep_expert, rows)

    sub = lax.broadcasted_iota(jnp.int32, (rows, rows), 0)
    lane = lax.broadcasted_iota(jnp.int32, (rows, rows), 1)

    def stacked(lines):
        out = jnp.zeros((rows, rows), F32)
        for i, line in enumerate(lines):
            out = jnp.where(sub == i, line, out)
        return jnp.transpose(out)

    route = routes[...].astype(F32)
    picks = [route[k : k + 1, :] for k in range(TOPK)]
    columns = stacked(picks)
    pick_cols = [columns[:, k : k + 1] for k in range(TOPK)]
    earlier = sub < lane
    group = jnp.floor((picks[0] + 0.5) / plane)
    group_col = jnp.floor((pick_cols[0] + 0.5) / plane)

    def tally(hits):
        return jnp.sum(jnp.where(hits & earlier, 1.0, 0.0), axis=0, keepdims=True)

    place = group * slots + tally(group_col == group)
    lines = []
    for k in range(TOPK):
        hits = pick_cols[0] == picks[k]
        for other in range(1, TOPK):
            hits = hits | (pick_cols[other] == picks[k])
        lines.append((picks[k] - group * plane) * cap + tally(hits) + 1.0)
        lines.append(group_weight[...] * pair_weight[k : k + 1, :])
    lines.append(place)
    columns = stacked(lines)
    n_slots = GROUPS * slots
    choose = jnp.where(
        lax.broadcasted_iota(jnp.int32, (n_slots, rows), 0).astype(F32) == place, 1.0, 0.0
    ).astype(BF16)
    place_col = columns[:, 2 * TOPK : 2 * TOPK + 1]
    choose_t[...] = jnp.where(
        lax.broadcasted_iota(jnp.int32, (rows, n_slots), 1).astype(F32) == place_col, 1.0, 0.0
    ).astype(BF16)
    details = dot(choose, columns.astype(BF16)).astype(BF16)
    meta_out[...] = details.reshape(meta_out.shape)
    meta_in[my_plane] = meta_out[my_plane]
    steps = [2, 1, 3] if GROUPS == 4 else list(range(1, GROUPS))
    meta_arrivals = [
        send(
            meta_out.at[(my_plane + step) % GROUPS], meta_in.at[my_plane], plane_peer(step)
        )
        for step in steps
    ]

    def z_copies(phase, c, source, target):
        target[c, my_plane] = source[c, my_plane]
        for step in steps:
            pltpu.make_async_remote_copy(
                src_ref=source.at[c, (my_plane + step) % GROUPS],
                dst_ref=target.at[c, my_plane],
                send_sem=z_send.at[phase, c],
                recv_sem=z_recv.at[phase, c],
                device_id=plane_peer(step),
                device_id_type=MESH,
            ).start()

    masks = range(plane - 1, 0, -1)
    across = [mask for mask in masks if mask % tp_count > 1]
    aside = [mask for mask in masks if mask % tp_count <= 1]

    def p_copies(phase, c, source, target, masks):
        for mask in masks:
            other = xor(my_place, mask)
            pltpu.make_async_remote_copy(
                src_ref=source.at[c, other],
                dst_ref=target.at[c, my_place],
                send_sem=p_send.at[phase, c],
                recv_sem=p_recv.at[phase, c],
                device_id=place_peer(other),
                device_id_type=MESH,
            ).start()

    def wait_all(buffer, c, blocks, sem):
        part = buffer.at[c, pl.ds(0, blocks)]
        pltpu.make_async_copy(part, part, sem).wait()

    for c in range(CHUNKS):
        value = dot(choose, normed[:, c * cols : (c + 1) * cols]).astype(BF16)
        packed[c] = value.reshape(packed.shape[1:])
        z_copies(0, c, packed, relayed)

    for name in others:
        loads[name].wait()
    sign = jnp.where(lax.broadcasted_iota(jnp.int32, (LOW, KEY_DIM), 1) < KEY_DIM // 2, -1.0, 1.0)

    @pl.loop(0, seg // LOW)
    def _(i):
        pair = coarse[i]
        at = pl.ds(pl.multiple_of(i * LOW, LOW), LOW)
        cosine[at, :] = pair[0:1] * fine[0] - pair[1:2] * fine[1]
        sine[at, :] = (pair[1:2] * fine[0] + pair[0:1] * fine[1]) * sign

    running = jnp.concatenate([decay[...], jnp.zeros((8 - heads, seg), F32)], axis=0)
    along = lax.broadcasted_iota(jnp.int32, running.shape, 1)
    shift = 1
    while shift < seg:
        running = running + jnp.where(along >= shift, pltpu.roll(running, shift, 1), 0.0)
        shift *= 2
    c_row[...] = running
    c_col[...] = jnp.transpose(running)

    n_out = 2 * keyw + 2 * valw
    tile = 256 if n_out % 256 == 0 else 128

    def weights():
        for name in ("wk", "wv", "wq", "wg"):
            loads[name].wait()

    def project(pair):
        at = pl.ds(pl.multiple_of(pair * 2 * rows, 2 * rows), 2 * rows)

        @pl.loop(0, n_out // tile)
        def _(n):
            part = pl.ds(pl.multiple_of(n * tile, tile), tile)
            lhs = mixer_rows[pl.ds(pair * 2, 2)].reshape(2 * rows, width)
            proj[at, part] = dot(lhs, w_all[:, part]).astype(BF16)

    order_of_steps = ORDER
    my_pair = tp // 2
    far_pairs = range(1, pairs)
    n_pos = plane * block
    ftile = 256

    def norm_block(place):
        def keep(at, value):
            mixer_rows[place, at, :] = value

        norm_rows(gathered.at[place], mixer_gain, keep, rows)

    def near_norm():
        norm_block(tp)
        near_arrival.wait_recv()
        norm_block(xor(tp, 1))

    def near_project():
        weights()
        project(my_pair)

    def spread_rows():
        for copy in meta_arrivals:
            copy.wait_recv()
        info = meta_in[...].reshape(n_slots, LANES).astype(F32)
        source = lax.broadcasted_iota(jnp.int32, (n_slots, 1), 0).astype(F32)
        source = jnp.floor((source + 0.5) / slots)
        position = lax.broadcasted_iota(jnp.int32, (n_slots, n_pos), 1).astype(F32)
        spread = jnp.zeros((n_slots, n_pos), F32)
        shares = jnp.zeros((n_slots, n_pos), F32)
        for k in range(TOPK):
            target = info[:, 2 * k : 2 * k + 1] - 1.0
            expert = jnp.floor((target + 0.5) / cap)
            there = expert * block + source * cap + (target - expert * cap)
            there = jnp.where(target >= 0.0, there, -1.0)
            hit = position == there
            spread = jnp.where(hit, 1.0, spread)
            shares = jnp.where(hit, info[:, 2 * k + 1 : 2 * k + 2], shares)
        mixing[...] = shares.astype(BF16)
        full = ceil_to(n_slots, LANES)
        if full > n_slots:
            spread = jnp.concatenate([spread, jnp.zeros((full - n_slots, n_pos), F32)], axis=0)
        spread_t[...] = jnp.transpose(spread)[:, :n_slots].astype(BF16)

    def relay(c):
        wait_all(relayed, c, GROUPS - 1, z_recv.at[0, c])
        value = dot(spread_t[...], relayed[c].reshape(n_slots, cols)).astype(BF16)
        sent[c] = value.reshape(sent.shape[1:])
        p_copies(0, c, sent, arrived, aside)
        arrived[c, my_place] = sent[c, my_place]

    def relay_far(c):
        p_copies(0, c, sent, arrived, across)

    passed = []

    def far_pass():
        for i in far_pairs:
            far_arrivals[i - 1].wait_recv()
            slot = gathered.at[xor(tp, 2 * i)]
            passed.append(send(slot, slot, {"tp": xor(tp, 1)}))

    def far_norm():
        for i in far_pairs:
            norm_block(xor(tp, 2 * i))
            passed[i - 1].wait_recv()
            norm_block(xor(tp, 2 * i + 1))

    def far_project():
        for i in far_pairs:
            project(xor(my_pair, i))

    def rotated(first):
        x = proj[:, first : first + KEY_DIM].astype(F32)
        return x * cosine[...] + pltpu.roll(x, KEY_DIM // 2, 1) * sine[...]

    def states():
        for h in range(heads):
            key = rotated(h * KEY_DIM).astype(BF16)
            proj[:, h * KEY_DIM : (h + 1) * KEY_DIM] = key
            total = c_row[h : h + 1, seg - 1 : seg]
            remain = jnp.exp(total - c_col[:, h : h + 1])
            weighted = (key.astype(F32) * remain).astype(BF16)
            values = proj[:, keyw + h * VALUE_DIM : keyw + (h + 1) * VALUE_DIM]
            state = lax.dot_general(
                weighted, values, (((0,), (0,)), ((), ())), preferred_element_type=F32
            )
            st_out[0, h * KEY_DIM : (h + 1) * KEY_DIM, :] = state.astype(BF16)
        tot_out[0] = jnp.broadcast_to(c_row[:, seg - 1 : seg], tot_out.shape[1:])
        st_in[inside] = st_out[0]
        tot_in[inside] = tot_out[0]
        for b, hop in enumerate(hops):
            @pl.when(my_plane < hop)
            def _():
                st_in[inner + b] = jnp.zeros(st_in.shape[1:], BF16)
                tot_in[inner + b] = jnp.zeros(tot_in.shape[1:], F32)

    arrivals = {}

    def state_send():
        arrivals[0] = []
        for j in range(1, inner):
            device = {"ep": my_plane * inner + (inside + j) % inner}
            arrivals[0].append(send(tot_out.at[0], tot_in.at[inside], device))
            arrivals[0].append(send(st_out.at[0], st_in.at[inside], device))

    def plane_send(b):
        if b < len(hops):
            device = {"ep": (ep + hops[b] * inner) % ep_count}
            goes = my_plane + hops[b] < GROUPS
            st_out[b + 1] = whole[...].astype(BF16)
            arrivals[b + 1] = [
                send(tot_out.at[b + 1], tot_in.at[inner + b], device, goes),
                send(st_out.at[b + 1], st_in.at[inner + b], device, goes),
            ]

    def state_plane():
        for copy in arrivals[0]:
            copy.wait_recv()
        total = tot_in[0]
        window = jnp.where(inside > 0, total, 0.0)
        for h in range(heads):
            at = slice(h * KEY_DIM, (h + 1) * KEY_DIM)
            part = st_in[0, at, :].astype(F32)
            whole[at, :] = part
            incoming[at, :] = jnp.where(inside > 0, part, 0.0)
        for i in range(1, inner):
            for h in range(heads):
                at = slice(h * KEY_DIM, (h + 1) * KEY_DIM)
                part = st_in[i, at, :].astype(F32)
                scale = jnp.exp(tot_in[i, h : h + 1, 0:1])
                whole[at, :] = part + scale * whole[at, :]
                if i < inner - 1:
                    joined = part + scale * incoming[at, :]
                    incoming[at, :] = jnp.where(inside > i, joined, incoming[at, :])
            total = total + tot_in[i]
            window = jnp.where(inside > i, window + tot_in[i], window)
        window_total[...] = window
        tot_out[1] = total
        plane_send(0)

    def state_hop(b):
        @pl.when(my_plane >= hops[b])
        def _():
            for copy in arrivals[b + 1]:
                copy.wait_recv()

        for h in range(heads):
            at = slice(h * KEY_DIM, (h + 1) * KEY_DIM)
            part = st_in[inner + b, at, :].astype(F32)
            incoming[at, :] = incoming[at, :] + jnp.exp(window_total[h : h + 1, 0:1]) * part
            if b + 1 < len(hops):
                scale = jnp.exp(tot_out[b + 1, h : h + 1, 0:1])
                whole[at, :] = whole[at, :] + scale * part
        window_total[...] = window_total[...] + tot_in[inner + b]
        if b + 1 < len(hops):
            tot_out[b + 2] = tot_out[b + 1] + tot_in[inner + b]
            plane_send(b + 1)

    def gate_up(c):
        if c == 0:
            loads["eg"].wait()
            loads["eu"].wait()
        group = range(sum(DEEP[:c]), sum(DEEP[: c + 1]))
        for i in group:
            wait_all(arrived, i, plane - 1, p_recv.at[0, i])

        @pl.loop(0, ff // ftile)
        def _(n):
            part = pl.ds(pl.multiple_of(n * ftile, ftile), ftile)
            upper = pl.ds(pl.multiple_of(ff + n * ftile, ftile), ftile)
            gate = acc[:, part] if c > 0 else 0.0
            up = acc[:, upper] if c > 0 else 0.0
            for i in group:
                lhs = arrived[i].reshape(n_pos, cols)
                deep = slice(i * cols, (i + 1) * cols)
                gate = gate + dot(lhs, eg[deep, part])
                up = up + dot(lhs, eu[deep, part])
            if c < len(DEEP) - 1:
                acc[:, part] = gate
                acc[:, upper] = up
            else:
                hidden[:, part] = (gate / (1.0 + jnp.exp(-gate)) * up).astype(BF16)

    def down(c):
        if c == 0:
            loads["ed"].wait()

        @pl.loop(0, cols // ftile)
        def _(n):
            part = pl.ds(pl.multiple_of(n * ftile, ftile), ftile)
            wide = pl.ds(pl.multiple_of(c * cols + n * ftile, ftile), ftile)
            value = dot(hidden[...], ed[:, wide]).astype(BF16)
            result[c, :, :, part] = value.reshape(plane, block, ftile)

        p_copies(1, c, result, returned, masks)
        returned[c, my_place] = result[c, my_place]

    def queries():
        loads["wo"].wait()
        for h in range(heads):
            first = keyw + valw + h * KEY_DIM
            proj[:, first : first + KEY_DIM] = rotated(first).astype(BF16)

    def retention(pair):
        base = pair * 2 * rows

        @pl.loop(0, 2)
        def _(b):
            start = pl.multiple_of(base + b * rows, rows)
            at = pl.ds(start, rows)
            t = start + lax.broadcasted_iota(jnp.int32, (rows, seg), 0)
            s = lax.broadcasted_iota(jnp.int32, (rows, seg), 1)
            for h in range(heads):
                first = keyw + valw + h * KEY_DIM
                query = proj[at, first : first + KEY_DIM]
                key = proj[:, h * KEY_DIM : (h + 1) * KEY_DIM]
                values = proj[:, keyw + h * VALUE_DIM : keyw + (h + 1) * VALUE_DIM]
                column = c_col[at, h : h + 1]
                gaps = column - c_row[h : h + 1, :]
                weight = jnp.where(t >= s, jnp.exp(jnp.minimum(gaps, 0.0)), 0.0)
                scores = lax.dot_general(
                    query, key, (((1,), (1,)), ((), ())), preferred_element_type=F32
                )
                scaled = (query.astype(F32) * jnp.exp(column)).astype(BF16)
                before = incoming[h * KEY_DIM : (h + 1) * KEY_DIM, :].astype(BF16)
                x = dot((scores * weight).astype(BF16), values) + dot(scaled, before)
                x = x - jnp.mean(x, axis=1, keepdims=True)
                spread = jnp.mean(x * x, axis=1, keepdims=True)
                wide = slice(h * VALUE_DIM, (h + 1) * VALUE_DIM)
                x = x * lax.rsqrt(spread + EPSILON) * head_gain[:, wide]
                first = 2 * keyw + valw + h * VALUE_DIM
                gate = proj[at, first : first + VALUE_DIM].astype(F32)
                gated[at, wide] = (gate / (1.0 + jnp.exp(-gate)) * x).astype(BF16)

        at = pl.ds(pl.multiple_of(base, 2 * rows), 2 * rows)

        @pl.loop(0, width // ftile)
        def _(n):
            part = pl.ds(pl.multiple_of(n * ftile, ftile), ftile)
            value = dot(gated[at, :], wo[:, part]).astype(BF16)
            terms[pl.ds(pair * 2, 2), :, part] = value.reshape(2, rows, ftile)

    def add_rows(store, parts):
        @pl.loop(0, rows // 32)
        def _(i):
            at = pl.ds(pl.multiple_of(i * 32, 32), 32)
            total = parts[0](at).astype(F32)
            for part in parts[1:]:
                total = total + part(at).astype(F32)
            store(at, total.astype(BF16))

    from_core = {}
    from_far = []

    def reduce_pair(i):
        pair = xor(my_pair, i)
        retention(pair)
        from_core[i] = send(terms.at[pair * 2 + 1 - core], pair_in.at[i], {"tp": xor(tp, 1)})

    def far_terms():
        for i in far_pairs:
            reduce_pair(i)

    def far_sums():
        for i in far_pairs:
            from_core[i].wait_recv()
            mine = xor(my_pair, i) * 2 + core

            def keep_far(at, value, i=i):
                far_out[i - 1, at, :] = value

            add_rows(keep_far, [
                lambda at, mine=mine: terms[mine, at, :], lambda at, i=i: pair_in[i, at, :]
            ])
            from_far.append(send(far_out.at[i - 1], far_in.at[i - 1], {"tp": xor(tp, 2 * i)}))

    def near_terms():
        reduce_pair(0)

    def combine(c):
        wait_all(returned, c, plane - 1, p_recv.at[1, c])
        value = dot(mixing[...], returned[c].reshape(n_pos, cols)).astype(BF16)
        combined[c] = value.reshape(combined.shape[1:])
        z_copies(1, c, combined, final)

    def finish(c):
        wait_all(final, c, GROUPS - 1, z_recv.at[1, c])
        value = dot(choose_t[...], final[c].reshape(n_slots, cols))
        expert_out[:, c * cols : (c + 1) * cols] = value.astype(BF16)

    def mixer_sum():
        from_core[0].wait_recv()
        for copy in from_far:
            copy.wait_recv()

        def keep_out(at, value):
            mixer_out[at, :] = value

        add_rows(keep_out, [
            lambda at: terms[tp, at, :], lambda at: pair_in[0, at, :]
        ] + [lambda at, i=i: far_in[i, at, :] for i in range(pairs - 1)])

    steps_by_name = locals()
    for name, *args in order_of_steps:
        steps_by_name[name](*args)

    for copy, when in singles:
        if when is None:
            copy.wait_send()
        else:
            pl.when(when)(copy.wait_send)
    for c in range(CHUNKS):
        wait_all(packed, c, GROUPS - 1, z_send.at[0, c])
        wait_all(combined, c, GROUPS - 1, z_send.at[1, c])
        wait_all(sent, c, plane - 1, p_send.at[0, c])
        wait_all(result, c, plane - 1, p_send.at[1, c])


def hand_out(mixed_in, expert_in, mixed_out, expert_out, sem):
    copies = [
        pltpu.make_async_copy(mixed_in, mixed_out, sem.at[0]),
        pltpu.make_async_copy(expert_in, expert_out, sem.at[1]),
    ]
    for copy in copies:
        copy.start()
    for copy in copies:
        copy.wait()


def local(
    ep_count, tp_count,
    mixer_input, log_decay, mixer_gain, query_weight, key_weight, value_weight, gate_weight,
    head_gain, output_weight, expert_input, expert_gain, routes, group_weight, pair_weight,
    expert_gate, expert_up, expert_down,
):
    rows, width = mixer_input.shape
    count = ep_count * tp_count
    plane = count // GROUPS
    cap = 3 * rows * TOPK // (2 * count)
    slots = ceil_to(plane * cap // TOPK, 16)
    block = ceil_to(cap * GROUPS, 16)
    cols = width // CHUNKS
    keyw = query_weight.shape[1]
    valw = value_weight.shape[1]
    heads = keyw // KEY_DIM
    seg = rows * tp_count
    ff = expert_gate.shape[2]
    n_slots = GROUPS * slots
    n_pos = plane * block
    pairs = tp_count // 2
    hops = (GROUPS - 1).bit_length()
    rounds = hops + 1
    distances = ep_count // GROUPS + hops
    coarse, fine = rope_tables(seg * ep_count)

    def buf(*shape, dtype=BF16):
        return pltpu.VMEM(shape, dtype)

    dma = pltpu.SemaphoreType.DMA
    scratch = [
        buf(heads, seg, dtype=F32), buf(1, width, dtype=F32), buf(1, valw, dtype=F32),
        buf(rows, width), buf(1, width, dtype=F32), buf(TOPK, rows, dtype=jnp.int32),
        buf(1, rows, dtype=F32), buf(TOPK, rows, dtype=F32),
        buf(seg // LOW, 2, KEY_DIM, dtype=F32), buf(2, LOW, KEY_DIM, dtype=F32),
        buf(tp_count, rows, width), buf(tp_count, rows, width),
        buf(width, 2 * keyw + 2 * valw), buf(valw, width),
        buf(width, ff), buf(width, ff), buf(ff, width),
        buf(seg, 2 * keyw + 2 * valw),
        buf(seg, KEY_DIM, dtype=F32), buf(seg, KEY_DIM, dtype=F32),
        buf(8, seg, dtype=F32), buf(seg, 8, dtype=F32),
        buf(rows, n_slots), buf(n_pos, n_slots), buf(n_slots, n_pos), buf(rows, width),
        buf(CHUNKS, GROUPS, slots, cols), buf(CHUNKS, GROUPS, slots, cols),
        buf(CHUNKS, plane, block, cols), buf(CHUNKS, plane, block, cols),
        buf(n_pos, 2 * ff, dtype=F32), buf(n_pos, ff),
        buf(CHUNKS, plane, block, cols), buf(CHUNKS, plane, block, cols),
        buf(CHUNKS, GROUPS, slots, cols), buf(CHUNKS, GROUPS, slots, cols),
        buf(GROUPS, slots, LANES), buf(GROUPS, slots, LANES),
        buf(rounds, keyw, VALUE_DIM), buf(distances, keyw, VALUE_DIM),
        buf(rounds, 8, LANES, dtype=F32), buf(distances, 8, LANES, dtype=F32),
        buf(keyw, VALUE_DIM, dtype=F32), buf(keyw, VALUE_DIM, dtype=F32), buf(8, LANES, dtype=F32),
        buf(seg, valw), buf(tp_count, rows, width), buf(pairs, rows, width),
        buf(max(1, pairs - 1), rows, width), buf(max(1, pairs - 1), rows, width),
        dma((20,)), dma((32,)), dma((32,)),
        dma((2, CHUNKS)), dma((2, CHUNKS)), dma((2, CHUNKS)), dma((2, CHUNKS)),
    ]
    any_space = pl.BlockSpec(memory_space=pl.ANY)
    vmem = pl.BlockSpec(memory_space=pltpu.VMEM)
    shape = jax.ShapeDtypeStruct((rows, width), BF16)
    outs = pl.pallas_call(
        functools.partial(body, (ep_count, tp_count, cap)),
        out_shape=(buf(rows, width), buf(rows, width)),
        in_specs=[any_space] * 19,
        out_specs=(vmem, vmem),
        scratch_shapes=scratch,
        compiler_params=pltpu.CompilerParams(
            collective_id=0, has_side_effects=True, vmem_limit_bytes=VMEM_LIMIT
        ),
    )(
        mixer_input, log_decay.T, mixer_gain[None, :], query_weight, key_weight, value_weight,
        gate_weight, head_gain[None, :], output_weight, expert_input, expert_gain[None, :],
        routes.T, group_weight[None, :], pair_weight.T, expert_gate, expert_up, expert_down,
        jnp.asarray(coarse), jnp.asarray(fine),
    )
    outs = [pltpu.with_memory_space_constraint(out, pltpu.VMEM) for out in outs]
    return pl.pallas_call(
        hand_out,
        out_shape=(shape, shape),
        in_specs=[vmem, vmem],
        out_specs=(any_space, any_space),
        scratch_shapes=[dma((2,))],
    )(*outs)


def solution(mesh):
    return jax.shard_map(
        functools.partial(local, mesh.shape["ep"], mesh.shape["tp"]),
        mesh=mesh,
        in_specs=(
            P(("ep", "tp"), None), P("ep", "tp"), P(), P(None, "tp"), P(None, "tp"),
            P(None, "tp"), P(None, "tp"), P("tp"), P("tp", None), P(("ep", "tp"), None), P(),
            P(("ep", "tp"), None), P(("ep", "tp")), P(("ep", "tp"), None),
            P(("ep", "tp"), None, None), P(("ep", "tp"), None, None),
            P(("ep", "tp"), None, None),
        ),
        out_specs=(P(("ep", "tp"), None), P(("ep", "tp"), None)),
        check_vma=False,
    )
```
